32 devices in a mesh: sp: 16 (over z, y, x), tp: 2 (over core).
Axes of the slice: x: 2, y: 2, z: 4, core: 2. Of those that a mesh axis runs over, the one named last changes fastest.
Arguments:
- queries: bfloat16 [4096, 1024], P('sp', 'tp'), may hold values from -12 to 12
- keys: bfloat16 [4096, 1024], P('sp', 'tp'), may hold values from -6 to 6
- values: bfloat16 [4096, 1024], P('sp', 'tp'), may hold values from -6 to 6
- w_out: bfloat16 [1024, 2048], P(None, 'tp'), may hold values from -0.375 to 0.375
Outputs:
- mixed: bfloat16 [4096, 2048], P('sp', 'tp')
The draws below stay inside these ranges and needn't reach their ends.
All inputs are finite; a program needn't handle non-finite values.
Results may differ from the reference program's by a relative error of at most 0.0056.
Values may be sent and summed in bfloat16 or wider, within the bound.
A program may use at most 64 MiB of HBM per device.

```python
import math
import jax
import jax.numpy as jnp
from jax import lax

HEADS = 8
HEAD_DIM = 128
D = 2048
SIDE_KEY_COUNT = 64
MIDDLE_DILATION = 4
FAR_DILATION = 16
TOKENS = 4096


def draw_queries(key, part):
    shape = (TOKENS, HEADS * HEAD_DIM)
    drawn = jnp.clip(2.0 * jax.random.normal(jax.random.fold_in(key, 1), shape, jnp.float32), -12.0, 12.0)
    return drawn.astype(jnp.bfloat16)


def draw_keys(key, part):
    shape = (TOKENS, HEADS * HEAD_DIM)
    drawn = jnp.clip(jax.random.normal(jax.random.fold_in(key, 2), shape, jnp.float32), -6.0, 6.0)
    return drawn.astype(jnp.bfloat16)


def levels(own_key, shape, split, least, largest):
    def one(dim, blocks):
        draws = jax.random.uniform(jax.random.fold_in(jax.random.fold_in(own_key, 6), dim), (blocks,), jnp.float32, least / len(split), largest / len(split))
        return jnp.repeat(jnp.exp(draws), shape[dim] // blocks).reshape((-1,) + (1,) * (len(shape) - dim - 1))

    loudness = one(*split[0])
    for cut in split[1:]:
        loudness = loudness * one(*cut)
    return loudness


def gaussian(own_key, shape, width, bound, cuts=(), kind=jnp.bfloat16):
    level = levels(own_key, shape, cuts, -0.22, 0.18) if cuts else 1.0
    values = jax.random.normal(own_key, shape, jnp.float32) * width * level
    return jnp.minimum(jnp.maximum(values, -bound), bound).astype(kind)


def setup_inputs(seed: int = 0) -> dict:
    key_of = jax.random.split(jax.random.key(seed), 5)
    queries = draw_queries(jax.random.fold_in(key_of[4], 71), 0)
    keys = draw_keys(jax.random.fold_in(key_of[4], 71), 0)
    values = gaussian(key_of[2], (TOKENS, HEADS * HEAD_DIM), 1.0, 6.0, ((0, 16), (1, 2)))
    w_out = gaussian(key_of[3], (HEADS * HEAD_DIM, D), (HEADS * HEAD_DIM // 4) ** -0.5, 0.375, ((1, 2),))
    return dict(queries=queries, keys=keys, values=values, w_out=w_out)


def block_rows(count):
    return count if count <= 128 else math.gcd(count, 128)


def band_scores(queries, keys, values, dilation_step):
    sequence_length, columns = queries.shape
    heads = columns // HEAD_DIM
    residue_rows = sequence_length // dilation_step
    rows_block = block_rows(residue_rows)
    blocks = residue_rows // rows_block
    span = rows_block + 2 * SIDE_KEY_COUNT
    padding = SIDE_KEY_COUNT * dilation_step
    padded_keys = jnp.pad(keys, ((padding, padding), (0, 0))).reshape(residue_rows + 2 * SIDE_KEY_COUNT, dilation_step, heads, HEAD_DIM)
    padded_values = jnp.pad(values, ((padding, padding), (0, 0))).reshape(residue_rows + 2 * SIDE_KEY_COUNT, dilation_step, heads, HEAD_DIM)
    grouped = queries.reshape(blocks, rows_block, dilation_step, heads, HEAD_DIM)
    query_idx = jnp.arange(rows_block, dtype=jnp.int32)[:, None]
    key_idx = jnp.arange(span, dtype=jnp.int32)[None, :]
    in_band = (key_idx >= query_idx) & (key_idx <= query_idx + 2 * SIDE_KEY_COUNT)
    residues = jnp.arange(dilation_step, dtype=jnp.int32)[:, None, None, None]
    scale = HEAD_DIM ** -0.5

    def one_block(inputs):
        number, query_block = inputs
        first_row = (number * rows_block).astype(jnp.int32)
        key_window = lax.dynamic_slice_in_dim(padded_keys, first_row, span, 0)
        value_window = lax.dynamic_slice_in_dim(padded_values, first_row, span, 0)
        scores = jnp.einsum('qrhe,krhe->rhqk', query_block.astype(jnp.float32), key_window.astype(jnp.float32)) * scale
        key_pos = (first_row + key_idx[None, None] - SIDE_KEY_COUNT) * dilation_step + residues
        allowed = in_band[None, None] & (key_pos >= 0) & (key_pos < sequence_length)
        scores = jnp.where(allowed, scores, -jnp.inf)
        maximum = jnp.max(scores, axis=-1, keepdims=True)
        raised = jnp.exp(scores - maximum)
        denominator = jnp.sum(raised, axis=-1, keepdims=True)
        weights = (raised / denominator).astype(jnp.bfloat16)
        attended = jnp.einsum('rhqk,krhe->qrhe', weights.astype(jnp.float32), value_window.astype(jnp.float32))
        log_den = (maximum + jnp.log(denominator))[..., 0]
        return attended, jnp.transpose(log_den, (2, 0, 1))

    outputs, log_dens = lax.map(one_block, (jnp.arange(blocks, dtype=jnp.int32), grouped))
    return outputs.reshape(sequence_length, heads, HEAD_DIM), log_dens.reshape(sequence_length, heads)


def reference(queries, keys, values, w_out):
    sequence_length, columns = queries.shape
    group_results = [band_scores(queries, keys, values, dilation_step) for dilation_step in (1, MIDDLE_DILATION, FAR_DILATION)]
    stacked_out = jnp.stack([item[0] for item in group_results])
    stacked_den = jnp.stack([item[1] for item in group_results])
    shares = jax.nn.softmax(stacked_den, axis=0)
    attended = jnp.sum(shares[..., None] * stacked_out, axis=0).astype(jnp.bfloat16).reshape(sequence_length, columns)
    return jnp.dot(attended, w_out, preferred_element_type=jnp.float32).astype(jnp.bfloat16)
```

```python
import functools
import math

import jax
import jax.numpy as jnp
from jax import lax
from jax.experimental import pallas as pl
from jax.experimental.pallas import tpu as pltpu
from jax.sharding import PartitionSpec as P

HEAD_DIM = 128
SIDE = 64
MID = 4
FAR = 16
MESH = pl.DeviceIdType.MESH
F32 = jnp.float32
BF16 = jnp.bfloat16
SCALE = HEAD_DIM ** -0.5 * math.log2(math.e)


def nt(a, b):
    return lax.dot_general(a, b, (((1,), (1,)), ((), ())), preferred_element_type=F32)


def nn(a, b):
    return lax.dot_general(a, b, (((1,), (0,)), ((), ())), preferred_element_type=F32)


def iota(shape, dim):
    return lax.broadcasted_iota(jnp.int32, shape, dim)


def attend(q, k, v, allowed):
    s = jnp.where(allowed, nt(q, k) * SCALE, -jnp.inf)
    top = jnp.max(s, axis=-1, keepdims=True)
    raised = jnp.exp2(s - top)
    den = jnp.sum(raised, axis=-1, keepdims=True)
    return nn(raised.astype(BF16), v), top, den


def kernel(sp_n, heads, q_hbm, k_hbm, v_hbm, out_ref,
           q_in, k_in, v_in, pkv, kvf, near_lo, near_hi, ob, ret, att, att_other, acc_n, md_n,
           relay, load_sem, hop_s, hop_r, kv_s, kv_r, q_s, q_r, up_s, up_r, dn_s, dn_r, near_s, near_r, ret_s, ret_r, tp_s, tp_r):
    rows = q_in.shape[0]
    chunk = rows // MID
    mm = rows // FAR
    e = HEAD_DIM
    p, c = lax.axis_index("sp"), lax.axis_index("tp")
    groups = sp_n // MID
    g, j = p // MID, p % MID

    loads = [
        pltpu.make_async_copy(src, dst, load_sem.at[n])
        for n, (src, dst) in enumerate(((k_hbm, k_in), (v_hbm, v_in), (q_hbm, q_in)))
    ]
    for load in loads:
        load.start()

    barrier = pltpu.get_barrier_semaphore()

    def greet(sp, tp):
        pl.semaphore_signal(barrier, inc=1, device_id=(sp, tp), device_id_type=MESH)

    def mate(d):
        return g * MID + (j + d) % MID

    for d in range(1, MID):
        greet(mate(d), c)
    greet(p, 1 - c)
    has_dn, has_up = g > 0, g < groups - 1
    has_prev, has_next = p > 0, p < sp_n - 1

    @pl.when(has_dn)
    def _():
        greet(p - MID, c)

    @pl.when(has_up)
    def _():
        greet(p + MID, c)

    @pl.when(has_prev)
    def _():
        greet(p - 1, c)

    @pl.when(has_next)
    def _():
        greet(p + 1, c)

    def remote(src, dst, ss, rs, sp, tp):
        return pltpu.make_async_remote_copy(
            src_ref=src, dst_ref=dst, send_sem=ss, recv_sem=rs, device_id=(sp, tp), device_id_type=MESH)

    r, t = iota((rows, rows), 0), iota((rows, rows), 1)
    perm = (t == FAR * (r % mm) + MID * ((r % chunk) // mm) + r // chunk).astype(BF16)
    r, t = t, r
    back = (t == FAR * (r % mm) + MID * ((r % chunk) // mm) + r // chunk).astype(BF16)

    for n, x in enumerate((k_in, v_in, q_in)):
        loads[n].wait()
        moved = nn(perm, x[...]).astype(BF16)
        for h in range(heads):
            pkv[h, n] = moved[:, h * e:(h + 1) * e]

    def at(n, base=0):
        return pl.ds(pl.multiple_of(base + n * chunk, chunk), chunk)

    for h in range(heads):
        for n in range(3):
            kvf[h, n, at(j, rows), :] = pkv[h, n, at(j), :]

    def edge(test, rows_at):
        @pl.when(jnp.logical_not(test))
        def _():
            for h in range(heads):
                for n in range(2):
                    kvf[h, n, pl.ds(rows_at, rows), :] = jnp.zeros((rows, e), BF16)

    edge(has_dn, 0)
    edge(has_up, 2 * rows)

    @pl.when(jnp.logical_not(has_prev))
    def _():
        near_lo[...] = jnp.zeros_like(near_lo)

    @pl.when(jnp.logical_not(has_next))
    def _():
        near_hi[...] = jnp.zeros_like(near_hi)

    pl.semaphore_wait(
        barrier,
        MID + has_dn.astype(jnp.int32) + has_up.astype(jnp.int32)
        + has_prev.astype(jnp.int32) + has_next.astype(jnp.int32))

    def up(h, d):
        n = (j - d + MID) % MID
        src = pkv.at[h, 0:2, at(n), :] if d == 0 else kvf.at[h, 0:2, at(n, rows), :]
        return remote(src, kvf.at[h, 0:2, at(n), :], up_s.at[h, d], up_r.at[h, d], (p + MID) % sp_n, c)

    def down(h, d):
        n = (j - d + MID) % MID
        src = pkv.at[h, 0:2, at(n), :] if d == 0 else kvf.at[h, 0:2, at(n, rows), :]
        return remote(src, kvf.at[h, 0:2, at(n, 2 * rows), :], dn_s.at[h, d], dn_r.at[h, d], (p - MID + sp_n) % sp_n, c)

    def forward(h, d):
        @pl.when(has_up)
        def _():
            up(h, d).start()

        @pl.when(has_dn)
        def _():
            down(h, d).start()

    def kv(h, d, receive=False):
        dst = (j - d + MID) % MID if receive else j
        return remote(pkv.at[h, 0:2, at((j + d) % MID), :], kvf.at[h, 0:2, at(dst, rows), :],
                      kv_s.at[h, d - 1], kv_r.at[h, d - 1], mate(d), c)

    def queries(d, receive=False):
        dst = (j - d + MID) % MID if receive else j
        return remote(pkv.at[:, 2, at((j + d) % MID), :], kvf.at[:, 2, at(dst, rows), :],
                      q_s.at[d - 1], q_r.at[d - 1], mate(d), c)

    for h in range(heads):
        for d in range(1, MID):
            kv(h, d).start()
        forward(h, 0)
    for d in range(1, MID):
        queries(d).start()

    def near(n, to_next):
        src = (k_in, v_in)[n]
        if to_next:
            return remote(src.at[pl.ds(rows - SIDE, SIDE), :], near_lo.at[n],
                          near_s.at[n, 0], near_r.at[n, 0], (p + 1) % sp_n, c)
        return remote(src.at[pl.ds(0, SIDE), :], near_hi.at[n],
                      near_s.at[n, 1], near_r.at[n, 1], (p - 1 + sp_n) % sp_n, c)

    def hop(side):
        first = (rows - SIDE, 0)[side]
        to = ((p + MID) % sp_n, (p - MID + sp_n) % sp_n)[side]
        return remote(v_in.at[pl.ds(first, SIDE), :], relay.at[side], near_s.at[1, side], hop_r.at[side], to, c)

    def pass_on(side):
        dst = (near_lo, near_hi)[side]
        return remote(relay.at[side], dst.at[1], hop_s.at[side], near_r.at[1, side], mate((1, MID - 1)[side]), c)

    @pl.when(has_next)
    def _():
        near(0, True).start()

    @pl.when(has_prev)
    def _():
        near(0, False).start()

    @pl.when(has_next & (j < MID - 1))
    def _():
        near(1, True).start()

    @pl.when(has_prev & (j > 0))
    def _():
        near(1, False).start()

    @pl.when(has_up & (j == MID - 1))
    def _():
        hop(0).start()

    @pl.when(has_dn & (j == 0))
    def _():
        hop(1).start()

    half = rows // 2
    own_span = half + SIDE
    qi, ki = iota((half, own_span), 0), iota((half, own_span), 1)
    for b in range(2):
        at_q = slice(b * half, (b + 1) * half)
        at_k = slice(b * (half - SIDE), b * (half - SIDE) + own_span)
        gap = (ki + at_k.start) - (qi + at_q.start)
        near_ok = (gap >= -SIDE) & (gap <= SIDE)
        for h in range(heads):
            cols = slice(h * e, (h + 1) * e)
            o, top, den = attend(q_in[at_q, cols], k_in[at_k, cols], v_in[at_k, cols], near_ok)
            acc_n[h, at_q, :] = o
            md_n[h, 0, at_q, :] = jnp.broadcast_to(top, (half, e))
            md_n[h, 1, at_q, :] = jnp.broadcast_to(den, (half, e))

    for h in range(heads):
        for d in range(1, MID):
            kv(h, d, receive=True).wait_recv()
            forward(h, d)

    relays = (has_dn & (j == MID - 1), has_up & (j == 0))
    for side in range(2):
        @pl.when(relays[side])
        def _():
            hop(side).wait_recv()
            pass_on(side).start()

    span = half + 2 * SIDE
    qi, ki = iota((half, span), 0), iota((half, span), 1)

    def order(x):
        return chunk * (x // chunk) + (FAR // MID) * (x % mm) + (x % chunk) // mm

    dn_ok, up_ok = has_dn.astype(jnp.int32), has_up.astype(jnp.int32)
    gap = order(ki) - order(qi)
    band = (gap >= 0) & (gap <= 2 * SIDE)
    mid_ok = (band & ((ki >= SIDE) | (dn_ok == 1)), band & ((ki < span - SIDE) | (up_ok == 1)))
    far_span, ns = 4 * chunk, FAR // MID
    ones = jnp.ones((far_span, e), BF16)
    qi, ki = iota((chunk, far_span), 0), iota((chunk, far_span), 1)
    far_ok = ((ki >= qi) & (ki <= qi + 2 * SIDE) & ((ki >= chunk) | (dn_ok == 1))
              & ((ki < 2 * chunk) | (up_ok == 1)))
    lane = iota((rows, e), 1)
    for d in range(1, MID):
        queries(d, receive=True).wait_recv()
    pick = (iota((16, e), 0) == iota((16, e), 1)).astype(BF16)

    def result(h, d, receive=False):
        dst = (j - d + MID) % MID if receive else j
        return remote(ob.at[h, (j + d) % MID], ret.at[h, dst],
                      ret_s.at[h, d - 1], ret_r.at[h, d - 1], mate(d), c)

    for h in range(heads):
        @pl.when(has_dn)
        def _():
            for d in range(MID):
                up(h, d).wait_recv()

        @pl.when(has_up)
        def _():
            for d in range(MID):
                down(h, d).wait_recv()

        q = kvf[h, 2, pl.ds(rows, rows), :]
        kh, vh = kvf[h, 0], kvf[h, 1]
        firsts = [rows - chunk + b * half for b in range(2)]
        s_mid = jnp.concatenate([
            jnp.where(mid_ok[b], nt(q[b * half:(b + 1) * half], kh[f:f + span]), -jnp.inf)
            for b, f in enumerate(firsts)], axis=0)
        q4 = q.reshape(MID, ns, mm, e)

        def classes(x):
            x4 = x.reshape(3 * MID, ns, mm, e)
            return [jnp.concatenate([x4[:, n], x4[:MID, n]], axis=0).reshape(far_span, e) for n in range(ns)]

        k_far, v_far = classes(kh), classes(vh)
        far = [jnp.where(far_ok, nt(q4[:, n].reshape(chunk, e), k_far[n]), -jnp.inf) for n in range(ns)]
        s_far = jnp.concatenate([far[n][i * mm:(i + 1) * mm] for i in range(MID) for n in range(ns)], axis=0)
        peak = functools.reduce(
            jnp.maximum, [x[:, i:i + e] for x in (s_mid, s_far) for i in range(0, x.shape[1], e)])
        top = jnp.max(peak, axis=-1, keepdims=True)
        r_mid = jnp.exp2((s_mid - top) * SCALE).astype(BF16)
        r_far = jnp.exp2((s_far - top) * SCALE).astype(BF16)
        total = jnp.concatenate([
            nn(r_mid[b * half:(b + 1) * half], jnp.concatenate([vh[f:f + span], ones], axis=1))
            for b, f in enumerate(firsts)], axis=0)
        far = [
            nn(jnp.concatenate([r_far[(i * ns + n) * mm:(i * ns + n + 1) * mm] for i in range(MID)], axis=0),
               jnp.concatenate([v_far[n], ones], axis=1))
            for n in range(ns)]
        total += jnp.concatenate([far[n][i * mm:(i + 1) * mm] for i in range(MID) for n in range(ns)], axis=0)
        den = total[:, e:]
        o = (total[:, :e] / den).astype(BF16)
        log_den = top * SCALE + jnp.log2(den)
        one = log_den.astype(BF16).astype(F32)
        two = (log_den - one).astype(BF16).astype(F32)
        three = log_den - one - two
        parts = jnp.where(lane == 0, one, jnp.where(lane == 1, two, three)).astype(BF16)
        twice = [parts[i * chunk:(i + 1) * chunk] for i in range(MID) for _ in range(2)]
        flat = nt(pick, jnp.concatenate(twice, axis=0)).astype(BF16)
        for i in range(MID):
            ob[h, i, :chunk] = o[i * chunk:(i + 1) * chunk]
            ob[h, i, chunk:] = flat[:, 2 * i * chunk:2 * (i + 1) * chunk]
        for d in range(1, MID):
            result(h, d).start()
        ret[h, pl.ds(j, 1)] = ob[h, pl.ds(j, 1)]

    @pl.when(has_prev)
    def _():
        for n in range(2):
            near(n, True).wait_recv()

    @pl.when(has_next)
    def _():
        for n in range(2):
            near(n, False).wait_recv()

    lo_ok, hi_ok = has_prev.astype(jnp.int32), has_next.astype(jnp.int32)
    qi, ki = iota((SIDE, SIDE), 0), iota((SIDE, SIDE), 1)
    corners = (
        (near_lo, slice(0, SIDE), (ki >= qi) & (lo_ok == 1)),
        (near_hi, slice(rows - SIDE, rows), (ki <= qi) & (hi_ok == 1)),
    )
    for h in range(heads):
        cols = slice(h * e, (h + 1) * e)
        for halo, at_q, ok in corners:
            s = jnp.where(ok, nt(q_in[at_q, cols], halo[0, :, cols]) * SCALE, -jnp.inf)
            old = md_n[h, 0, at_q, :]
            top = jnp.maximum(old, jnp.max(s, axis=-1, keepdims=True))
            fade = jnp.exp2(old - top)
            raised = jnp.exp2(s - top[:, :SIDE])
            acc_n[h, at_q, :] = fade * acc_n[h, at_q, :] + nn(raised.astype(BF16), halo[1, :, cols])
            md_n[h, 0, at_q, :] = top
            md_n[h, 1, at_q, :] = fade * md_n[h, 1, at_q, :] + jnp.sum(raised, axis=-1, keepdims=True)

    r, t = iota((rows, 2 * rows), 1), iota((rows, 2 * rows), 0)
    low = r % (2 * chunk) < chunk
    r = r // (2 * chunk) * chunk + r % (2 * chunk)
    back_twice = (low & (t == FAR * (r % mm) + MID * ((r % chunk) // mm) + r // chunk)).astype(BF16)

    def share(h):
        cols = pl.ds(h * e, e)
        return remote(att.at[:, cols], att_other.at[:, cols], tp_s.at[h], tp_r.at[h], p, 1 - c)

    for h in range(heads):
        for d in range(1, MID):
            result(h, d, receive=True).wait_recv()
        o = nn(back, jnp.concatenate([ret[h, i, :chunk] for i in range(MID)], axis=0))
        parts = nt(back_twice, jnp.concatenate([ret[h, i, chunk:] for i in range(MID)], axis=1))
        log_den = parts[:, 0:1] + parts[:, 1:2] + parts[:, 2:3]
        t_n, d_n = md_n[h, 0], md_n[h, 1]
        top = jnp.maximum(t_n, log_den)
        e1, e2 = jnp.exp2(t_n - top), jnp.exp2(log_den - top)
        att[:, h * e:(h + 1) * e] = ((e1 * acc_n[h] + e2 * o) / (e1 * d_n + e2)).astype(BF16)
        share(h).start()

    width = heads * e
    out_ref[:, pl.ds(pl.multiple_of(c * width, width), width)] = att[...]
    for h in range(heads):
        share(h).wait_recv()
        out_ref[:, pl.ds(pl.multiple_of((1 - c) * width + h * e, e), e)] = att_other[:, h * e:(h + 1) * e]

    for h in range(heads):
        for d in range(1, MID):
            kv(h, d).wait_send()
            result(h, d).wait_send()
        share(h).wait_send()
    for d in range(1, MID):
        queries(d).wait_send()
    for side in range(2):
        @pl.when(relays[side])
        def _():
            pass_on(side).wait_send()
    @pl.when(has_up)
    def _():
        for h in range(heads):
            for d in range(MID):
                up(h, d).wait_send()

    @pl.when(has_dn)
    def _():
        for h in range(heads):
            for d in range(MID):
                down(h, d).wait_send()

    @pl.when(has_next)
    def _():
        for n in range(2):
            near(n, True).wait_send()

    @pl.when(has_prev)
    def _():
        for n in range(2):
            near(n, False).wait_send()


def per_device(sp_n, q, k, v, w):
    rows, columns = q.shape
    heads = columns // HEAD_DIM
    assert MID * rows == SIDE * FAR and rows // MID == SIDE and sp_n % MID == 0
    dma = pltpu.SemaphoreType.DMA
    e, chunk = HEAD_DIM, rows // MID
    attended = pl.pallas_call(
        functools.partial(kernel, sp_n, heads),
        out_shape=pltpu.VMEM((rows, w.shape[0]), BF16),
        in_specs=[pl.BlockSpec(memory_space=pltpu.HBM)] * 3,
        out_specs=pl.BlockSpec(memory_space=pltpu.VMEM),
        scratch_shapes=[
            pltpu.VMEM((rows, columns), BF16),
            pltpu.VMEM((rows, columns), BF16),
            pltpu.VMEM((rows, columns), BF16),
            pltpu.VMEM((heads, 3, rows, e), BF16),
            pltpu.VMEM((heads, 3, 3 * rows, e), BF16),
            pltpu.VMEM((2, SIDE, columns), BF16),
            pltpu.VMEM((2, SIDE, columns), BF16),
            pltpu.VMEM((heads, MID, chunk + 16, e), BF16),
            pltpu.VMEM((heads, MID, chunk + 16, e), BF16),
            pltpu.VMEM((rows, columns), BF16),
            pltpu.VMEM((rows, columns), BF16),
            pltpu.VMEM((heads, rows, e), F32),
            pltpu.VMEM((heads, 2, rows, e), F32),
            pltpu.VMEM((2, SIDE, columns), BF16),
            dma((3,)),
            dma((2,)), dma((2,)),
            dma((heads, MID - 1)), dma((heads, MID - 1)),
            dma((MID - 1,)), dma((MID - 1,)),
            dma((heads, MID)), dma((heads, MID)),
            dma((heads, MID)), dma((heads, MID)),
            dma((2, 2)), dma((2, 2)),
            dma((heads, MID - 1)), dma((heads, MID - 1)),
            dma((heads,)), dma((heads,)),
        ],
        compiler_params=pltpu.CompilerParams(collective_id=0, has_side_effects=True, vmem_limit_bytes=40*1024*1024),
    )(*[pltpu.with_memory_space_constraint(x, pltpu.HBM) for x in (q, k, v)])
    return nn(attended, w).astype(BF16)


def solution(mesh):
    return jax.shard_map(
        functools.partial(per_device, mesh.shape["sp"]), mesh=mesh,
        in_specs=(P("sp", "tp"), P("sp", "tp"), P("sp", "tp"), P(None, "tp")),
        out_specs=P("sp", "tp"), check_vma=False,
    )
```

```python
import functools
import math

import jax
import jax.numpy as jnp
from jax import lax
from jax.experimental import pallas as pl
from jax.experimental.pallas import tpu as pltpu
from jax.sharding import PartitionSpec as P

HEAD_DIM = 128
SIDE = 64
MID = 4
FAR = 16
NS = FAR // MID
MESH = pl.DeviceIdType.MESH
F32 = jnp.float32
BF16 = jnp.bfloat16
SCALE = HEAD_DIM ** -0.5 * math.log2(math.e)
NEG = -jnp.inf


def nt(a, b):
    return lax.dot_general(a, b, (((1,), (1,)), ((), ())), preferred_element_type=F32)


def nn(a, b):
    return lax.dot_general(a, b, (((1,), (0,)), ((), ())), preferred_element_type=F32)


def iota(shape, dim):
    return lax.broadcasted_iota(jnp.int32, shape, dim)


def bias(ok):
    return jnp.where(ok, 0.0, NEG).astype(F32)


def kernel(sp_n, heads, q_hbm, k_hbm, v_hbm, w_hbm, out_ref,
           q_in, k_in, v_in, w_in, ps, kv, qp, edge_in, edge_out, ends, near_bias, mid_bias, far_bias, rim_bias,
           o_s, t_s, d_s, ob, att, ys,
           load_sem, kv_s, kv_r, q_s, q_r, up_s, up_r, dn_s, dn_r, ei_s, ei_r, eo_s, eo_r,
           res_s, res_r, cross_s, cross_r, tp_s, tp_r):
    rows = q_in.shape[0]
    chunk = rows // MID
    mm = rows // FAR
    e = HEAD_DIM
    width = heads * e
    last = MID - 1
    p, c = lax.axis_index("sp"), lax.axis_index("tp")
    groups = sp_n // MID
    g, j = p // MID, p % MID

    loads = [
        pltpu.make_async_copy(src, dst, load_sem.at[n])
        for n, (src, dst) in enumerate(((k_hbm, k_in), (v_hbm, v_in), (q_hbm, q_in), (w_hbm, w_in)))
    ]
    for load in loads:
        load.start()

    barrier = pltpu.get_barrier_semaphore()

    def greet(sp, tp):
        pl.semaphore_signal(barrier, inc=1, device_id=(sp, tp), device_id_type=MESH)

    def mate(d):
        return g * MID + (j + d) % MID

    for d in range(1, MID):
        greet(mate(d), c)
        greet(mate(d), 1 - c)
    greet(p, 1 - c)
    has_dn, has_up = g > 0, g < groups - 1

    @pl.when(has_dn)
    def _():
        greet(p - MID, c)

    @pl.when(has_up)
    def _():
        greet(p + MID, c)

    def remote(src, dst, ss, rs, sp, tp):
        return pltpu.make_async_remote_copy(
            src_ref=src, dst_ref=dst, send_sem=ss, recv_sem=rs, device_id=(sp, tp), device_id_type=MESH)

    def token(r):
        return FAR * (r % mm) + MID * ((r % chunk) // mm) + r // chunk

    r, t = iota((rows, rows), 0), iota((rows, rows), 1)
    perm = (t == token(r)).astype(BF16)
    back = (r == token(t)).astype(BF16)

    for n, x in enumerate((k_in, v_in, q_in)):
        loads[n].wait()
        moved = nn(perm, x[...]).astype(BF16)
        for h in range(heads):
            for m in range(MID):
                ps[m, h, n] = moved[m * chunk:(m + 1) * chunk, h * e:(h + 1) * e]

    up_p, dn_p = (p + MID) % sp_n, (p - MID + sp_n) % sp_n
    has = (has_up, has_dn)

    @pl.when(jnp.logical_not(has_dn))
    def _():
        kv[0] = jnp.zeros(kv.shape[1:], BF16)
        edge_out[0] = jnp.zeros(edge_out.shape[1:], BF16)

    @pl.when(jnp.logical_not(has_up))
    def _():
        kv[2] = jnp.zeros(kv.shape[1:], BF16)
        edge_out[1] = jnp.zeros(edge_out.shape[1:], BF16)

    pl.semaphore_wait(barrier, 2 * MID - 1 + has_dn.astype(jnp.int32) + has_up.astype(jnp.int32))

    def give(m, d, receive=False):
        dst = (j - d + MID) % MID if receive else j
        return remote(ps.at[m, (j + d) % MID, pl.ds(0, 2)], kv.at[1, m, :, dst],
                      kv_s.at[m, d - 1], kv_r.at[m, d - 1], mate(d), c)

    def ask(i, d, receive=False):
        dst = (j - d + MID) % MID if receive else j
        two = pl.ds(2 * i, 2)
        return remote(ps.at[two, (j + d) % MID, 2], qp.at[two, dst],
                      q_s.at[i, d - 1], q_r.at[i, d - 1], mate(d), c)

    def up(m, d):
        n = (j - d + MID) % MID
        src = ps.at[m, j, pl.ds(0, 2)] if d == 0 else kv.at[1, m, :, n]
        return remote(src, kv.at[0, m, :, n], up_s.at[m, d], up_r.at[m, d], up_p, c)

    def down(m, d):
        n = (j - d + MID) % MID
        src = ps.at[m, j, pl.ds(0, 2)] if d == 0 else kv.at[1, m, :, n]
        return remote(src, kv.at[2, m, :, n], dn_s.at[m, d], dn_r.at[m, d], dn_p, c)

    def forward(m, d):
        @pl.when(has_up)
        def _():
            up(m, d).start()

        @pl.when(has_dn)
        def _():
            down(m, d).start()

    homes = (j == last, j == 0)
    firsts = (rows - SIDE, 0)
    out_p = (up_p, dn_p)

    def rim_in(side, n, d):
        src = (k_in, v_in)[n].at[pl.ds(firsts[side], SIDE), pl.ds(pl.multiple_of((j + d) % MID * e, e), e)]
        return remote(src, edge_in.at[side, n], ei_s.at[side, n, d - 1], ei_r.at[side, n], mate(d), c)

    def rim_out(side, n, home):
        src = (k_in, v_in)[n].at[pl.ds(firsts[side], SIDE), pl.ds(pl.multiple_of(j * e, e), e)] if home else edge_in.at[side, n]
        return remote(src, edge_out.at[side, n], eo_s.at[side, n], eo_r.at[side, n], out_p[side], c)

    def give_all(m):
        for d in range(1, MID):
            give(m, d).start()

    def ask_all(i):
        for d in range(1, MID):
            ask(i, d).start()

    give_all(0)
    for m in range(MID):
        forward(m, 0)
    give_all(1)
    for side in range(2):
        @pl.when(has[side] & homes[side])
        def _():
            for n in range(2):
                for d in range(1, MID):
                    rim_in(side, n, d).start()
                rim_out(side, n, True).start()
    ask_all(0)
    give_all(2)
    give_all(3)
    ask_all(1)

    for m in range(MID):
        kv[1, m, :, pl.ds(j, 1)] = ps[m, pl.ds(j, 1), 0:2].reshape(2, 1, chunk, e)
        qp[m, pl.ds(j, 1)] = ps[m, pl.ds(j, 1), 2]

    ok_dn, ok_up = has_dn.astype(jnp.int32) == 1, has_up.astype(jnp.int32) == 1
    tq, s = token(iota((rows, rows), 0)), iota((rows, rows), 1)
    gap = tq - token(s)
    near_bias[:, :rows] = bias((gap >= -SIDE) & (gap <= SIDE))
    tq, s = token(iota((rows, 2 * SIDE), 0)), iota((rows, 2 * SIDE), 1)
    near_bias[:, rows:] = bias(((s < SIDE) & (s >= tq)) | ((s >= SIDE) & (s - SIDE <= tq - (rows - SIDE))))

    def order(x):
        return chunk * (x // chunk) + NS * (x % mm) + (x % chunk) // mm

    half = rows // 2
    uq, uk = order(iota((half, 3 * chunk), 0)), order(iota((half, 3 * chunk), 1))
    for i in range(2):
        gap = uk - uq - i * chunk
        mid_bias[i] = bias((gap >= -SIDE) & (gap <= SIDE))
    x, s = iota((chunk, 2 * chunk), 0), iota((chunk, 2 * chunk), 1)
    far_bias[...] = bias(((s < chunk) & (s >= x) & ok_dn) | ((s >= chunk) & (s - chunk <= x) & ok_up))
    x, s = iota((half, 2 * chunk), 0), iota((half, 2 * chunk), 1)
    u, v = order(x % chunk), order(s % chunk)
    rim_bias[...] = bias(((x < chunk) & (s < chunk) & (v >= u) & ok_dn)
                         | ((x >= chunk) & (s >= chunk) & (v <= u) & ok_up))

    def collect(m):
        for d in range(1, MID):
            give(m, d, receive=True).wait_recv()
            forward(m, d)

    def classes(x):
        x4 = x.reshape(MID, NS, mm, e)
        return [x4[:, n].reshape(chunk, e) for n in range(NS)]

    def unclass(parts):
        return jnp.concatenate([parts[n][i * mm:(i + 1) * mm] for i in range(MID) for n in range(NS)], axis=0)

    def with_ones(x):
        return jnp.concatenate([x, jnp.ones((x.shape[0], e), BF16)], axis=1)

    def prob(s, top):
        return jnp.exp2((s - top) * SCALE).astype(BF16)

    def home_plane(m):
        q = qp[m].reshape(rows, e)
        kh, vh = kv[1, m, 0].reshape(rows, e), kv[1, m, 1].reshape(rows, e)
        mid = [nt(q[i * half:(i + 1) * half], kh[i * chunk:(i + 3) * chunk]) + mid_bias[i] for i in range(2)]
        mid = jnp.concatenate(mid, axis=0)
        far = unclass([nt(a, b) for a, b in zip(classes(q), classes(kh))])
        top = jnp.maximum(
            jnp.max(mid[:, :2 * chunk], axis=-1, keepdims=True),
            jnp.max(jnp.maximum(mid[:, 2 * chunk:], far), axis=-1, keepdims=True))
        p_mid, p_far = prob(mid, top), prob(far, top)
        total = jnp.concatenate([
            nn(p_mid[i * half:(i + 1) * half], with_ones(vh[i * chunk:(i + 3) * chunk])) for i in range(2)], axis=0)
        p4 = p_far.reshape(MID, NS, mm, chunk)
        total += unclass([nn(p4[:, n].reshape(chunk, chunk), with_ones(v)) for n, v in enumerate(classes(vh))])
        o_s[m] = total[:, :e].reshape(MID, chunk, e)
        d_s[m] = total[:, e:].reshape(MID, chunk, e)
        t_s[m] = jnp.broadcast_to(top, (rows, e)).reshape(MID, chunk, e)

    def find_ends():
        x, s = iota((2 * SIDE, rows), 0), iota((2 * SIDE, rows), 1)
        pick = (token(s) == x + (x // SIDE) * (rows - 2 * SIDE)).astype(BF16)
        for b in range(MID):
            both = jnp.concatenate([kv[1, :, 0, b].reshape(rows, e), kv[1, :, 1, b].reshape(rows, e)], axis=1)
            both = nn(pick, both).astype(BF16)
            for side in range(2):
                for n in range(2):
                    ends[side, b, n] = both[side * SIDE:(side + 1) * SIDE, n * e:(n + 1) * e]

    lane = iota((1, 2 * SIDE), 1)

    def near(b):
        q = qp[:, b].reshape(rows, e)
        kb, vb = kv[1, :, 0, b].reshape(rows, e), kv[1, :, 1, b].reshape(rows, e)
        lo = [ends[1, b - 1, n] if b > 0 else edge_out[0, n] for n in range(2)]
        hi = [ends[0, b + 1, n] if b < last else edge_out[1, n] for n in range(2)]
        k_rim, v_rim = (jnp.concatenate([lo[n], hi[n]], axis=0) for n in range(2))
        own = nt(q, kb) + near_bias[:, :rows]
        rim = nt(q, k_rim) + near_bias[:, rows:]
        if b == 0:
            rim += bias((lane >= SIDE) | ok_dn)
        if b == last:
            rim += bias((lane < SIDE) | ok_up)
        old = t_s[:, b].reshape(rows, e)
        peak = jnp.maximum(jnp.maximum(own[:, :e], own[:, e:]), rim)
        top = jnp.maximum(old, jnp.max(peak, axis=-1, keepdims=True))
        fade = jnp.exp2((old - top) * SCALE)
        both = jnp.concatenate([top, top], axis=1)
        total = nn(prob(own, both), with_ones(vb)) + nn(prob(rim, top), with_ones(v_rim))
        o_s[:, b] = (fade * o_s[:, b].reshape(rows, e) + total[:, :e]).reshape(MID, chunk, e)
        d_s[:, b] = (fade * d_s[:, b].reshape(rows, e) + total[:, e:]).reshape(MID, chunk, e)
        t_s[:, b] = top.reshape(MID, chunk, e)

    def other_planes(m):
        q = qp[m].reshape(rows, e)
        k2 = [[kv[i, m, n].reshape(rows, e) for n in range(2)] for i in (0, 2)]
        cat = lambda a, b: jnp.concatenate([a, b], axis=0)
        k_far = [cat(a, b) for a, b in zip(classes(k2[0][0]), classes(k2[1][0]))]
        v_far = [cat(a, b) for a, b in zip(classes(k2[0][1]), classes(k2[1][1]))]
        far = unclass([nt(a, b) + far_bias[...] for a, b in zip(classes(q), k_far)])
        k_rim, v_rim = (cat(k2[0][n][last * chunk:], k2[1][n][:chunk]) for n in range(2))
        rim = nt(cat(q[:chunk], q[last * chunk:]), k_rim) + rim_bias[...]
        peak = jnp.concatenate([
            jnp.maximum(far[:chunk], rim[:chunk]), far[chunk:last * chunk],
            jnp.maximum(far[last * chunk:], rim[chunk:])], axis=0)
        old = t_s[m].reshape(rows, e)
        top = jnp.maximum(old, jnp.max(peak, axis=-1, keepdims=True))
        fade = jnp.exp2((old - top) * SCALE)
        p4 = prob(far, top).reshape(MID, NS, mm, 2 * chunk)
        total = unclass([nn(p4[:, n].reshape(chunk, 2 * chunk), with_ones(v)) for n, v in enumerate(v_far)])
        extra = nn(prob(rim, cat(top[:chunk], top[last * chunk:])), with_ones(v_rim))
        total = jnp.concatenate([
            total[:chunk] + extra[:chunk], total[chunk:last * chunk], total[last * chunk:] + extra[chunk:]], axis=0)
        o = fade * o_s[m].reshape(rows, e) + total[:, :e]
        den = fade * d_s[m].reshape(rows, e) + total[:, e:]
        ob[m] = (o / den).astype(BF16).reshape(MID, chunk, e)

    def cols(core, head):
        return pl.ds(pl.multiple_of(core * width + head * e, e), e)

    def result(m, d, receive=False):
        head = (j - d + MID) % MID if receive else j
        return remote(ob.at[m, (j + d) % MID], att.at[m, :, cols(c, head)],
                      res_s.at[m, d - 1], res_r.at[m, d - 1], mate(d), c)

    def across(d, receive=False):
        core, head = (1 - c, (j - d + MID) % MID) if receive else (c, j)
        return remote(ob.at[last, (j + d) % MID], att.at[last, :, cols(core, head)],
                      cross_s.at[d], cross_r.at[d], mate(d), 1 - c)

    def share(m):
        side = pl.ds(pl.multiple_of(c * width, width), width)
        return remote(att.at[m, :, side], att.at[m, :, side], tp_s.at[m], tp_r.at[m], p, 1 - c)

    def share_in(m):
        side = pl.ds(pl.multiple_of((1 - c) * width, width), width)
        return remote(att.at[m, :, side], att.at[m, :, side], tp_s.at[m], tp_r.at[m], p, 1 - c)

    def finish(m):
        @pl.when(has_dn)
        def _():
            for d in range(MID):
                up(m, d).wait_recv()

        @pl.when(has_up)
        def _():
            for d in range(MID):
                down(m, d).wait_recv()

        other_planes(m)
        for d in range(1, MID):
            result(m, d).start()
        if m == last:
            for d in range(MID):
                across(d).start()
        att[m, :, cols(c, j)] = ob[m, pl.ds(j, 1)].reshape(chunk, e)

    collect(0)
    collect(1)
    for side in range(2):
        @pl.when(has[side] & jnp.logical_not(homes[side]))
        def _():
            for n in range(2):
                rim_in(side, n, 1).wait_recv()
                rim_out(side, n, False).start()
    for d in range(1, MID):
        ask(0, d, receive=True).wait_recv()
    home_plane(0)
    collect(2)
    home_plane(1)
    collect(3)
    for d in range(1, MID):
        ask(1, d, receive=True).wait_recv()
    home_plane(2)
    home_plane(3)
    find_ends()
    for side in range(2):
        @pl.when(has[1 - side])
        def _():
            for n in range(2):
                rim_out(side, n, False).wait_recv()
    for b in range(MID):
        near(b)
    for m in range(MID):
        finish(m)

    for m in range(last):
        for d in range(1, MID):
            result(m, d, receive=True).wait_recv()
        share(m).start()
    loads[3].wait()
    for m in range(last):
        share_in(m).wait_recv()
    ys[:last * chunk] = nn(att[:last].reshape(last * chunk, 2 * width), w_in[...]).astype(BF16)
    for d in range(1, MID):
        result(last, d, receive=True).wait_recv()
    for d in range(MID):
        across(d, receive=True).wait_recv()
    ys[last * chunk:] = nn(att[last], w_in[...]).astype(BF16)
    out_ref[...] = nn(back, ys[...]).astype(BF16)

    for m in range(MID):
        for d in range(1, MID):
            give(m, d).wait_send()
            result(m, d).wait_send()
    for d in range(MID):
        across(d).wait_send()
    for m in range(last):
        share(m).wait_send()
    for i in range(2):
        for d in range(1, MID):
            ask(i, d).wait_send()

    @pl.when(has_up)
    def _():
        for m in range(MID):
            for d in range(MID):
                up(m, d).wait_send()

    @pl.when(has_dn)
    def _():
        for m in range(MID):
            for d in range(MID):
                down(m, d).wait_send()

    for side in range(2):
        @pl.when(has[side])
        def _():
            for n in range(2):
                rim_out(side, n, False).wait_send()

        @pl.when(has[side] & homes[side])
        def _():
            for n in range(2):
                for d in range(1, MID):
                    rim_in(side, n, d).wait_send()


def per_device(sp_n, q, k, v, w):
    rows, columns = q.shape
    heads = columns // HEAD_DIM
    assert MID * rows == SIDE * FAR and rows // MID == SIDE and sp_n % MID == 0 and heads == MID
    dma = pltpu.SemaphoreType.DMA
    e, chunk = HEAD_DIM, rows // MID
    vmem = lambda *shape, dtype=BF16: pltpu.VMEM(shape, dtype)
    pinned = [pltpu.with_memory_space_constraint(x, pltpu.HBM) for x in (q, k, v, w)]
    return pl.pallas_call(
        functools.partial(kernel, sp_n, heads),
        out_shape=pltpu.VMEM((rows, w.shape[1]), BF16),
        in_specs=[pl.BlockSpec(memory_space=pltpu.HBM)] * 4,
        out_specs=pl.BlockSpec(memory_space=pltpu.VMEM),
        scratch_shapes=[
            vmem(rows, columns), vmem(rows, columns), vmem(rows, columns), vmem(*w.shape),
            vmem(MID, heads, 3, chunk, e),
            vmem(3, MID, 2, MID, chunk, e),
            vmem(MID, MID, chunk, e),
            vmem(2, 2, SIDE, e), vmem(2, 2, SIDE, e),
            vmem(2, MID, 2, SIDE, e),
            vmem(rows, rows + 2 * SIDE, dtype=F32),
            vmem(2, rows // 2, 3 * chunk, dtype=F32),
            vmem(chunk, 2 * chunk, dtype=F32),
            vmem(rows // 2, 2 * chunk, dtype=F32),
            vmem(MID, MID, chunk, e, dtype=F32), vmem(MID, MID, chunk, e, dtype=F32), vmem(MID, MID, chunk, e, dtype=F32),
            vmem(MID, MID, chunk, e),
            vmem(MID, chunk, 2 * columns),
            vmem(rows, w.shape[1]),
            dma((4,)),
            dma((MID, MID - 1)), dma((MID, MID - 1)),
            dma((2, MID - 1)), dma((2, MID - 1)),
            dma((MID, MID)), dma((MID, MID)),
            dma((MID, MID)), dma((MID, MID)),
            dma((2, 2, MID - 1)), dma((2, 2)),
            dma((2, 2)), dma((2, 2)),
            dma((MID, MID - 1)), dma((MID, MID - 1)),
            dma((MID,)), dma((MID,)),
            dma((MID,)), dma((MID,)),
        ],
        compiler_params=pltpu.CompilerParams(
            collective_id=0, has_side_effects=True, vmem_limit_bytes=40 * 1024 * 1024),
    )(*pinned)


def solution(mesh):
    return jax.shard_map(
        functools.partial(per_device, mesh.shape["sp"]), mesh=mesh,
        in_specs=(P("sp", "tp"), P("sp", "tp"), P("sp", "tp"), P(None, "tp")),
        out_specs=P("sp", "tp"), check_vma=False,
    )
```

```python
import functools
import math

import jax
import jax.numpy as jnp
from jax import lax
from jax.experimental import pallas as pl
from jax.experimental.pallas import tpu as pltpu
from jax.sharding import PartitionSpec as P

HEAD_DIM = 128
SIDE = 64
MID = 4
FAR = 16
NS = FAR // MID
MESH = pl.DeviceIdType.MESH
F32 = jnp.float32
BF16 = jnp.bfloat16
SCALE = HEAD_DIM ** -0.5 * math.log2(math.e)
NEG = -jnp.inf
EARLY = 2


def nt(a, b):
    return lax.dot_general(a, b, (((1,), (1,)), ((), ())), preferred_element_type=F32)


def nn(a, b):
    return lax.dot_general(a, b, (((1,), (0,)), ((), ())), preferred_element_type=F32)


def iota(shape, dim):
    return lax.broadcasted_iota(jnp.int32, shape, dim)


def bias(ok):
    return jnp.where(ok, 0.0, NEG).astype(F32)


def kernel(sp_n, heads, q_hbm, k_hbm, v_hbm, w_hbm, out_ref,
           q_in, k_in, v_in, w_in, ps, kv, qp, ends, outer, near_bias, mid_bias, far_bias, rim_bias,
           o_s, t_s, d_s, ob, att, natural,
           load_sem, give_s, give_r, ask_s, ask_r, up_s, up_r, dn_s, dn_r, res_s, res_r, cross_s, cross_r, tp_s, tp_r):
    rows = q_in.shape[0]
    chunk = rows // MID
    mm = rows // FAR
    e = HEAD_DIM
    width = heads * e
    last = MID - 1
    p, c = lax.axis_index("sp"), lax.axis_index("tp")
    groups = sp_n // MID
    g, j = p // MID, p % MID

    loads = [
        pltpu.make_async_copy(src, dst, load_sem.at[n])
        for n, (src, dst) in enumerate(((k_hbm, k_in), (v_hbm, v_in), (q_hbm, q_in), (w_hbm, w_in)))
    ]
    for load in loads[:3]:
        load.start()

    barrier = pltpu.get_barrier_semaphore()

    def greet(sp, tp):
        pl.semaphore_signal(barrier, inc=1, device_id=(sp, tp), device_id_type=MESH)

    others = (MID - 1 - j, j + 1 - 2 * (j % 2), (j + MID // 2) % MID)

    def mate(d):
        return g * MID + others[d]

    for d in range(last):
        greet(mate(d), c)
        greet(mate(d), 1 - c)
    greet(p, 1 - c)
    has_dn, has_up = g > 0, g < groups - 1
    up_p, dn_p = (p + MID) % sp_n, (p - MID + sp_n) % sp_n

    @pl.when(has_dn)
    def _():
        greet(dn_p, c)

    @pl.when(has_up)
    def _():
        greet(up_p, c)

    def remote(src, dst, ss, rs, sp, tp):
        return pltpu.make_async_remote_copy(
            src_ref=src, dst_ref=dst, send_sem=ss, recv_sem=rs, device_id=(sp, tp), device_id_type=MESH)

    def await_all(ref, sem):
        pltpu.make_async_copy(ref, ref, sem).wait()

    def token(r):
        return FAR * (r % mm) + MID * ((r % chunk) // mm) + r // chunk

    r, t = iota((rows, rows), 0), iota((rows, rows), 1)
    perm = (t == token(r)).astype(BF16)

    def reorder(n, x):
        loads[n].wait()
        moved = nn(perm, x[...]).astype(BF16)
        for h in range(heads):
            for m in range(MID):
                ps[m, h, n] = moved[m * chunk:(m + 1) * chunk, h * e:(h + 1) * e]

    reorder(0, k_in)
    reorder(1, v_in)

    @pl.when(jnp.logical_not(has_dn))
    def _():
        kv[0] = jnp.zeros(kv.shape[1:], BF16)

    @pl.when(jnp.logical_not(has_up))
    def _():
        kv[2] = jnp.zeros(kv.shape[1:], BF16)

    pl.semaphore_wait(barrier, 2 * MID - 1 + has_dn.astype(jnp.int32) + has_up.astype(jnp.int32))

    pair = pl.ds(0, 2)

    def give(m, d):
        return remote(ps.at[m, others[d], pair], kv.at[1, m, :, j], give_s.at[0], give_r.at[m, j], mate(d), c)

    def ask(i, d):
        two = pl.ds(2 * i, 2)
        return remote(ps.at[two, others[d], 2], qp.at[two, j], ask_s.at[0], ask_r.at[i], mate(d), c)

    def up(m, b, own=False):
        src = ps.at[m, j, pair] if own else kv.at[1, m, :, b]
        arrived = (b == last).astype(jnp.int32) * MID + (b != last).astype(jnp.int32) * m if own else (MID if b == last else m)
        return remote(src, kv.at[0, m, :, b], up_s.at[0], up_r.at[arrived], up_p, c)

    def down(m, b, own=False):
        src = ps.at[m, j, pair] if own else kv.at[1, m, :, b]
        arrived = (b == 0).astype(jnp.int32) * MID + (b != 0).astype(jnp.int32) * m if own else (MID if b == 0 else m)
        return remote(src, kv.at[2, m, :, b], dn_s.at[0], dn_r.at[arrived], dn_p, c)

    for m in range(MID):
        for d in range(last):
            give(m, d).start()
        if m == 0:
            @pl.when(has_up)
            def _():
                for i in range(MID):
                    up(i, j, own=True).start()

            @pl.when(has_dn)
            def _():
                for i in range(MID):
                    down(i, j, own=True).start()

    reorder(2, q_in)
    for i in range(2):
        for d in range(last):
            ask(i, d).start()

    loads[3].start()
    for m in range(MID):
        kv[1, m, :, pl.ds(j, 1)] = ps[m, pl.ds(j, 1), 0:2].reshape(2, 1, chunk, e)
        qp[m, pl.ds(j, 1)] = ps[m, pl.ds(j, 1), 2]

    ok_dn, ok_up = has_dn.astype(jnp.int32) == 1, has_up.astype(jnp.int32) == 1
    tq, s = token(iota((rows, rows), 0)), iota((rows, rows), 1)
    gap = tq - token(s)
    near_bias[:, :rows] = bias((gap >= -SIDE) & (gap <= SIDE))
    tq, s = token(iota((rows, 2 * SIDE), 0)), iota((rows, 2 * SIDE), 1)
    near_bias[:, rows:] = bias(((s < SIDE) & (s >= tq)) | ((s >= SIDE) & (s - SIDE <= tq - (rows - SIDE))))

    def order(x):
        return chunk * (x // chunk) + NS * (x % mm) + (x % chunk) // mm

    half = rows // 2
    uq, uk = order(iota((half, 3 * chunk), 0)), order(iota((half, 3 * chunk), 1))
    for i in range(2):
        gap = uk - uq - i * chunk
        mid_bias[i] = bias((gap >= -SIDE) & (gap <= SIDE))
    x, s = iota((chunk, 2 * chunk), 0), iota((chunk, 2 * chunk), 1)
    far_bias[...] = bias(((s < chunk) & (s >= x) & ok_dn) | ((s >= chunk) & (s - chunk <= x) & ok_up))
    x, s = iota((half, 2 * chunk), 0), iota((half, 2 * chunk), 1)
    u, v = order(x % chunk), order(s % chunk)
    low, high = (x < chunk) & (s < chunk) & ok_dn, (x >= chunk) & (s >= chunk) & ok_up
    for m in range(MID):
        tq = token(m * chunk + x % chunk)
        rim_bias[m, :, :2 * chunk] = bias((low & (v >= u)) | (high & (v <= u)))
        rim_bias[m, :, 2 * chunk:] = bias((low & (s >= tq)) | (high & (s - SIDE <= tq - (rows - SIDE))))

    def arrival(m, b, rise, fall):
        @pl.when(j != b)
        def _():
            await_all(kv.at[1, m, :, b], give_r.at[m, b])

        relay(m, b, rise, fall)

    def relay(m, b, rise, fall):
        if rise:
            @pl.when((j != b) & has_up)
            def _():
                up(m, b).start()

        if fall:
            @pl.when((j != b) & has_dn)
            def _():
                down(m, b).start()

    def classes(x):
        x4 = x.reshape(MID, NS, mm, e)
        return [x4[:, n].reshape(chunk, e) for n in range(NS)]

    def unclass(parts):
        return jnp.concatenate([parts[n][i * mm:(i + 1) * mm] for i in range(MID) for n in range(NS)], axis=0)

    def cat(*parts):
        return jnp.concatenate(parts, axis=0)

    def with_ones(x):
        return jnp.concatenate([x, jnp.ones((x.shape[0], e), BF16)], axis=1)

    def prob(s, top):
        return jnp.exp2((s - top) * SCALE).astype(BF16)

    x, s = iota((2 * SIDE, rows), 0), iota((2 * SIDE, rows), 1)
    pick = (token(s) == x + (x // SIDE) * (rows - 2 * SIDE)).astype(BF16)

    def both(i, b):
        return jnp.concatenate([kv[i, :, n, b].reshape(rows, e) for n in range(2)], axis=1)

    def find_ends():
        for b in range(MID):
            x = nn(pick, both(1, b)).astype(BF16)
            for side in range(2):
                for n in range(2):
                    ends[side, b, n] = x[side * SIDE:(side + 1) * SIDE, n * e:(n + 1) * e]

    def find_outer():
        x = cat(nn(pick[SIDE:], both(0, last)), nn(pick[:SIDE], both(2, 0))).astype(BF16)
        for n in range(2):
            outer[n] = x[:, n * e:(n + 1) * e]

    lane = iota((1, 2 * SIDE), 1)

    def middle(m):
        q = qp[m].reshape(rows, e)
        kh, vh = kv[1, m, 0].reshape(rows, e), kv[1, m, 1].reshape(rows, e)
        mid = cat(*[nt(q[i * half:(i + 1) * half], kh[i * chunk:(i + 3) * chunk]) + mid_bias[i] for i in range(2)])
        top = jnp.maximum(jnp.max(mid[:, :e], axis=-1, keepdims=True), jnp.max(mid[:, e:], axis=-1, keepdims=True))
        p_mid = prob(mid, top)
        total = cat(*[nn(p_mid[i * half:(i + 1) * half], with_ones(vh[i * chunk:(i + 3) * chunk])) for i in range(2)])
        o_s[m] = total[:, :e]
        d_s[m] = total[:, e:]
        t_s[m] = jnp.broadcast_to(top, (rows, e))

    def near(b):
        q = qp[:, b].reshape(rows, e)
        kb, vb = kv[1, :, 0, b].reshape(rows, e), kv[1, :, 1, b].reshape(rows, e)
        k_rim, v_rim = (cat(ends[1, max(b - 1, 0), n], ends[0, min(b + 1, last), n]) for n in range(2))
        own = nt(q, kb) + near_bias[:, :rows]
        rim = nt(q, k_rim) + near_bias[:, rows:]
        if b == 0:
            rim += bias(lane >= SIDE)
        if b == last:
            rim += bias(lane < SIDE)
        at_b = pl.ds(b * chunk, chunk)
        old = t_s[:, at_b].reshape(rows, e)
        peak = jnp.maximum(jnp.maximum(own[:, :e], own[:, e:]), rim)
        top = jnp.maximum(old, jnp.max(peak, axis=-1, keepdims=True))
        fade = jnp.exp2((old - top) * SCALE)
        both = jnp.concatenate([top, top], axis=1)
        total = nn(prob(own, both), with_ones(vb)) + nn(prob(rim, top), with_ones(v_rim))
        o_s[:, at_b] = (fade * o_s[:, at_b].reshape(rows, e) + total[:, :e]).reshape(MID, chunk, e)
        d_s[:, at_b] = (fade * d_s[:, at_b].reshape(rows, e) + total[:, e:]).reshape(MID, chunk, e)
        t_s[:, at_b] = top.reshape(MID, chunk, e)

    def other_planes(m):
        q = qp[m].reshape(rows, e)
        k2 = [[kv[i, m, n].reshape(rows, e) for n in range(2)] for i in (0, 2, 1)]
        k_far, v_far = ([cat(*x) for x in zip(*(classes(k2[i][n]) for i in range(3)))] for n in range(2))
        far = [nt(a, b) for a, b in zip(classes(q), k_far)]
        near_far, own = unclass([x[:, :e] + far_bias[...] for x in far]), unclass([x[:, e:] for x in far])
        far = near_far
        k_rim, v_rim = (cat(k2[0][n][last * chunk:], k2[1][n][:chunk], outer[n]) for n in range(2))
        rim = nt(cat(q[:chunk], q[last * chunk:]), k_rim) + rim_bias[m]
        peak = jnp.maximum(rim[:, :e], rim[:, e:])
        peak = cat(jnp.maximum(far[:chunk], peak[:chunk]), far[chunk:last * chunk],
                   jnp.maximum(far[last * chunk:], peak[chunk:]))
        old = t_s[m]
        top = jnp.maximum(old, jnp.maximum(
            jnp.max(peak, axis=-1, keepdims=True), jnp.max(own, axis=-1, keepdims=True)))
        fade = jnp.exp2((old - top) * SCALE)
        p4 = jnp.concatenate([prob(far, top), prob(own, top[:, :chunk])], axis=1).reshape(MID, NS, mm, 3 * chunk)
        total = unclass([nn(p4[:, n].reshape(chunk, 3 * chunk), with_ones(v)) for n, v in enumerate(v_far)])
        top = cat(top[:chunk], top[last * chunk:])
        extra = nn(prob(rim, jnp.concatenate([top, top], axis=1)), with_ones(v_rim))
        total = cat(total[:chunk] + extra[:chunk], total[chunk:last * chunk], total[last * chunk:] + extra[chunk:])
        o = fade * o_s[m] + total[:, :e]
        den = fade * d_s[m] + total[:, e:]
        ob[m] = (o / den).astype(BF16).reshape(MID, chunk, e)

    def cols(core, head):
        return pl.ds(pl.multiple_of(core * width + head * e, e), e)

    def side(core):
        return pl.ds(pl.multiple_of(core * width, width), width)

    def result(m, d):
        return remote(ob.at[m, others[d]], att.at[m, :, cols(c, j)], res_s.at[0], res_r.at[m], mate(d), c)

    def across(m, b, to):
        return remote(ob.at[m, b], att.at[m, :, cols(c, j)], cross_s.at[0], cross_r.at[m - EARLY], to, 1 - c)

    def share(m):
        return remote(att.at[m, :, side(c)], att.at[m, :, side(c)], tp_s.at[0], tp_r.at[max(m - EARLY + 1, 0)], p, 1 - c)

    early = tuple(range(EARLY))
    late = tuple(range(EARLY, MID))

    def finish(ms):
        @pl.when(has_dn)
        def _():
            for m in ms:
                await_all(kv.at[0, m, :, pl.ds(0, last)], up_r.at[m])

        @pl.when(has_up)
        def _():
            for m in ms:
                await_all(kv.at[2, m, :, pl.ds(1, last)], dn_r.at[m])

        for m in ms:
            other_planes(m)
        for m in ms:
            for d in range(last):
                result(m, d).start()
            if m in late:
                @pl.when(c == 0)
                def _():
                    for d in range(last):
                        across(m, others[d], mate(d)).start()
                    across(m, j, p).start()
            att[m, :, cols(c, j)] = ob[m, pl.ds(j, 1)].reshape(chunk, e)

    def project(ms):
        y = nn(att[ms[0]:ms[-1] + 1].reshape(len(ms) * chunk, 2 * width), w_in[...])
        for i, m in enumerate(ms):
            for n in range(NS):
                part = y[i * chunk + n * mm:i * chunk + (n + 1) * mm]
                for t in range(natural.shape[0]):
                    natural[t, pl.ds(MID * n + m, mm, stride=FAR), :] = part[:, t * e:(t + 1) * e]

    for b in range(MID):
        arrival(0, b, True, True)
    for b in range(MID):
        arrival(1, b, True, True)
    for b in range(MID):
        arrival(2, b, b == last, b == 0)
    for b in range(MID):
        arrival(3, b, b == last, b == 0)
    for m in range(2, MID):
        for b in range(MID):
            relay(m, b, b != last, b != 0)
    find_ends()
    await_all(qp.at[pl.ds(0, 2), pl.ds(0, last)], ask_r.at[0])
    middle(0)
    middle(1)
    await_all(qp.at[pl.ds(0, 2), pl.ds(0, last)], ask_r.at[1])
    middle(2)
    middle(3)
    for b in range(MID):
        near(b)
    @pl.when(has_dn)
    def _():
        await_all(kv.at[0, :, :, last], up_r.at[MID])

    @pl.when(has_up)
    def _():
        await_all(kv.at[2, :, :, 0], dn_r.at[MID])

    find_outer()
    finish((0, 1))
    finish((2,))
    finish((3,))
    for m in early:
        await_all(ob.at[m, pl.ds(0, last)], res_r.at[m])
        share(m).start()
    loads[3].wait()
    def project_early():
        await_all(att.at[pl.ds(0, EARLY), :, side(1 - c)], tp_r.at[0])
        project(early)

    @pl.when(c == 0)
    def _():
        project_early()
        for m in late:
            await_all(ob.at[m, pl.ds(0, last)], res_r.at[m])
            await_all(att.at[m, :, side(1 - c)], tp_r.at[m - EARLY + 1])
            project((m,))

    @pl.when(c == 1)
    def _():
        for m in late:
            await_all(ob.at[m, pl.ds(0, last)], res_r.at[m])
            share(m).start()
        for m in late:
            await_all(ob.at[m], cross_r.at[m - EARLY])
            project((m,))
        project_early()

    for t in range(natural.shape[0]):
        out_ref[:, t * e:(t + 1) * e] = natural[t].astype(BF16)

    await_all(ps.at[:, pl.ds(0, last), pair], give_s.at[0])
    await_all(ps.at[:, pl.ds(0, last), 2], ask_s.at[0])
    await_all(ob.at[:, pl.ds(0, last)], res_s.at[0])

    @pl.when(c == 0)
    def _():
        await_all(ob.at[pl.ds(0, MID - EARLY)], cross_s.at[0])
        await_all(att.at[pl.ds(0, EARLY), :, side(c)], tp_s.at[0])

    @pl.when(c == 1)
    def _():
        await_all(att.at[:, :, side(c)], tp_s.at[0])

    @pl.when(has_up)
    def _():
        await_all(kv.at[0], up_s.at[0])

    @pl.when(has_dn)
    def _():
        await_all(kv.at[2], dn_s.at[0])


def per_device(sp_n, q, k, v, w):
    rows, columns = q.shape
    heads = columns // HEAD_DIM
    assert MID * rows == SIDE * FAR and rows // MID == SIDE and sp_n % MID == 0 and heads == MID
    dma = pltpu.SemaphoreType.DMA
    e, chunk = HEAD_DIM, rows // MID
    vmem = lambda *shape, dtype=BF16: pltpu.VMEM(shape, dtype)
    pinned = [pltpu.with_memory_space_constraint(x, pltpu.HBM) for x in (q, k, v, w)]
    return pl.pallas_call(
        functools.partial(kernel, sp_n, heads),
        out_shape=pltpu.VMEM((rows, w.shape[1]), BF16),
        in_specs=[pl.BlockSpec(memory_space=pltpu.HBM)] * 4,
        out_specs=pl.BlockSpec(memory_space=pltpu.VMEM),
        scratch_shapes=[
            vmem(rows, columns), vmem(rows, columns), vmem(rows, columns), vmem(*w.shape),
            vmem(MID, heads, 3, chunk, e),
            vmem(3, MID, 2, MID, chunk, e),
            vmem(MID, MID, chunk, e),
            vmem(2, MID, 2, SIDE, e),
            vmem(2, 2 * SIDE, e),
            vmem(rows, rows + 2 * SIDE, dtype=F32),
            vmem(2, rows // 2, 3 * chunk, dtype=F32),
            vmem(chunk, 2 * chunk, dtype=F32),
            vmem(MID, rows // 2, 4 * chunk, dtype=F32),
            vmem(MID, rows, e, dtype=F32), vmem(MID, rows, e, dtype=F32), vmem(MID, rows, e, dtype=F32),
            vmem(MID, MID, chunk, e),
            vmem(MID, chunk, 2 * columns),
            vmem(w.shape[1] // e, rows, e, dtype=F32),
            dma((4,)),
            dma((1,)), dma((MID, MID)),
            dma((1,)), dma((2,)),
            dma((1,)), dma((MID + 1,)),
            dma((1,)), dma((MID + 1,)),
            dma((1,)), dma((MID,)),
            dma((1,)), dma((MID - EARLY,)),
            dma((1,)), dma((MID - EARLY + 1,)),
        ],
        compiler_params=pltpu.CompilerParams(
            collective_id=0, has_side_effects=True, vmem_limit_bytes=40 * 1024 * 1024),
    )(*pinned)


def solution(mesh):
    return jax.shard_map(
        functools.partial(per_device, mesh.shape["sp"]), mesh=mesh,
        in_specs=(P("sp", "tp"), P("sp", "tp"), P("sp", "tp"), P(None, "tp")),
        out_specs=P("sp", "tp"), check_vma=False,
    )
```

```python
import functools
import math

import jax
import jax.numpy as jnp
from jax import lax
from jax.experimental import pallas as pl
from jax.experimental.pallas import tpu as pltpu
from jax.sharding import PartitionSpec as P

HEAD_DIM = 128
SIDE = 64
MID = 4
FAR = 16
NS = FAR // MID
MESH = pl.DeviceIdType.MESH
F32 = jnp.float32
BF16 = jnp.bfloat16
SCALE = HEAD_DIM ** -0.5 * math.log2(math.e)
NEG = -jnp.inf
EARLY = 2


def nt(a, b):
    return lax.dot_general(a, b, (((1,), (1,)), ((), ())), preferred_element_type=F32)


def nn(a, b):
    return lax.dot_general(a, b, (((1,), (0,)), ((), ())), preferred_element_type=F32)


def iota(shape, dim):
    return lax.broadcasted_iota(jnp.int32, shape, dim)


def bias(ok):
    return jnp.where(ok, 0.0, NEG).astype(F32)


def kernel(sp_n, heads, q_hbm, k_hbm, v_hbm, w_hbm, out_ref,
           q_in, k_in, v_in, w_in, ps, kv, qp, ends, outer, near_bias, mid_bias, far_bias, rim_bias,
           o_s, t_s, d_s, ob, att, partial, natural,
           load_sem, give_s, give_r, ask_s, ask_r, up_s, up_r, dn_s, dn_r, res_s, res_r, cross_s, cross_r, tp_s, tp_r):
    rows = q_in.shape[0]
    chunk = rows // MID
    mm = rows // FAR
    e = HEAD_DIM
    width = heads * e
    last = MID - 1
    p, c = lax.axis_index("sp"), lax.axis_index("tp")
    groups = sp_n // MID
    g, j = p // MID, p % MID

    loads = [
        pltpu.make_async_copy(src, dst, load_sem.at[n])
        for n, (src, dst) in enumerate(((k_hbm, k_in), (v_hbm, v_in), (q_hbm, q_in), (w_hbm, w_in)))
    ]
    for load in loads[:3]:
        load.start()

    barrier = pltpu.get_barrier_semaphore()

    def greet(sp, tp):
        pl.semaphore_signal(barrier, inc=1, device_id=(sp, tp), device_id_type=MESH)

    others = (MID - 1 - j, j + 1 - 2 * (j % 2), (j + MID // 2) % MID)

    def mate(d):
        return g * MID + others[d]

    for d in range(last):
        greet(mate(d), c)
        greet(mate(d), 1 - c)
    greet(p, 1 - c)
    has_dn, has_up = g > 0, g < groups - 1
    up_p, dn_p = (p + MID) % sp_n, (p - MID + sp_n) % sp_n

    @pl.when(has_dn)
    def _():
        greet(dn_p, c)

    @pl.when(has_up)
    def _():
        greet(up_p, c)

    def remote(src, dst, ss, rs, sp, tp):
        return pltpu.make_async_remote_copy(
            src_ref=src, dst_ref=dst, send_sem=ss, recv_sem=rs, device_id=(sp, tp), device_id_type=MESH)

    def await_all(ref, sem):
        pltpu.make_async_copy(ref, ref, sem).wait()

    def token(r):
        return FAR * (r % mm) + MID * ((r % chunk) // mm) + r // chunk

    r, t = iota((rows, rows), 0), iota((rows, rows), 1)
    perm = (t == token(r)).astype(BF16)

    def reorder(*arrays):
        for n, _ in arrays:
            loads[n].wait()
        for n, x in arrays:
            moved = nn(perm, x[...]).astype(BF16)
            for h in range(heads):
                for m in range(MID):
                    ps[m, h, n] = moved[m * chunk:(m + 1) * chunk, h * e:(h + 1) * e]

    reorder((0, k_in), (1, v_in))

    @pl.when(jnp.logical_not(has_dn))
    def _():
        kv[0] = jnp.zeros(kv.shape[1:], BF16)

    @pl.when(jnp.logical_not(has_up))
    def _():
        kv[2] = jnp.zeros(kv.shape[1:], BF16)

    pl.semaphore_wait(barrier, 2 * MID - 1 + has_dn.astype(jnp.int32) + has_up.astype(jnp.int32))

    pair = pl.ds(0, 2)

    def give(m, d):
        return remote(ps.at[m, others[d], pair], kv.at[1, m, :, j], give_s.at[0], give_r.at[j if m == 0 else last + m], mate(d), c)

    def ask(i, d):
        two = pl.ds(2 * i, 2)
        return remote(ps.at[two, others[d], 2], qp.at[two, j], ask_s.at[0], ask_r.at[i], mate(d), c)

    def up(m, b, own=False):
        src = ps.at[m, j, pair] if own else kv.at[1, m, :, b]
        edge = (b == last).astype(jnp.int32) if hasattr(b, "astype") else int(b == last)
        arrived = edge * MID + (1 - edge) * m
        return remote(src, kv.at[0, m, :, b], up_s.at[0], up_r.at[arrived], up_p, c)

    def down(m, b, own=False):
        src = ps.at[m, j, pair] if own else kv.at[1, m, :, b]
        edge = (b == 0).astype(jnp.int32) if hasattr(b, "astype") else int(b == 0)
        arrived = edge * MID + (1 - edge) * m
        return remote(src, kv.at[2, m, :, b], dn_s.at[0], dn_r.at[arrived], dn_p, c)

    for m in range(MID):
        for d in ((1, 2, 0) if m == 0 else range(last)):
            give(m, d).start()
        if m == 0:
            @pl.when(has_up)
            def _():
                for i in range(MID):
                    up(i, j, own=True).start()

            @pl.when(has_dn)
            def _():
                for i in range(MID):
                    down(i, j, own=True).start()

    reorder((2, q_in))
    for i in range(2):
        for d in range(last):
            ask(i, d).start()

    loads[3].start()
    for m in range(MID):
        kv[1, m, :, pl.ds(j, 1)] = ps[m, pl.ds(j, 1), 0:2].reshape(2, 1, chunk, e)
        qp[m, pl.ds(j, 1)] = ps[m, pl.ds(j, 1), 2]

    ok_dn, ok_up = has_dn.astype(jnp.int32) == 1, has_up.astype(jnp.int32) == 1
    tq, s = token(iota((rows, rows), 0)), iota((rows, rows), 1)
    gap = tq - token(s)
    near_bias[:, :rows] = bias((gap >= -SIDE) & (gap <= SIDE))
    tq, s = token(iota((rows, 2 * SIDE), 0)), iota((rows, 2 * SIDE), 1)
    near_bias[:, rows:] = bias(((s < SIDE) & (s >= tq)) | ((s >= SIDE) & (s - SIDE <= tq - (rows - SIDE))))

    def order(x):
        return chunk * (x // chunk) + NS * (x % mm) + (x % chunk) // mm

    half = rows // 2
    uq, uk = order(iota((half, 3 * chunk), 0)), order(iota((half, 3 * chunk), 1))
    for i in range(2):
        gap = uk - uq - i * chunk
        mid_bias[i] = bias((gap >= -SIDE) & (gap <= SIDE))
    x, s = iota((chunk, 2 * chunk), 0), iota((chunk, 2 * chunk), 1)
    far_bias[...] = bias(((s < chunk) & (s >= x) & ok_dn) | ((s >= chunk) & (s - chunk <= x) & ok_up))
    x, s = iota((half, 2 * chunk), 0), iota((half, 2 * chunk), 1)
    u, v = order(x % chunk), order(s % chunk)
    low, high = (x < chunk) & (s < chunk) & ok_dn, (x >= chunk) & (s >= chunk) & ok_up
    for m in range(MID):
        tq = token(m * chunk + x % chunk)
        rim_bias[m, :, :2 * chunk] = bias((low & (v >= u)) | (high & (v <= u)))
        rim_bias[m, :, 2 * chunk:] = bias((low & (s >= tq)) | (high & (s - SIDE <= tq - (rows - SIDE))))

    def relay(m, b, rise, fall):
        if rise:
            @pl.when((j != b) & has_up)
            def _():
                up(m, b).start()

        if fall:
            @pl.when((j != b) & has_dn)
            def _():
                down(m, b).start()

    def classes(x):
        x4 = x.reshape(MID, NS, mm, e)
        return [x4[:, n].reshape(chunk, e) for n in range(NS)]

    def unclass(parts):
        return jnp.concatenate([parts[n][i * mm:(i + 1) * mm] for i in range(MID) for n in range(NS)], axis=0)

    def cat(*parts):
        return jnp.concatenate(parts, axis=0)

    def with_ones(x):
        return jnp.concatenate([x, jnp.ones((x.shape[0], e), BF16)], axis=1)

    def prob(s, top):
        return jnp.exp2((s - top) * SCALE).astype(BF16)

    x, s = iota((2 * SIDE, rows), 0), iota((2 * SIDE, rows), 1)
    pick = (token(s) == x + (x // SIDE) * (rows - 2 * SIDE)).astype(BF16)

    def both(i, b):
        return jnp.concatenate([kv[i, :, n, b].reshape(rows, e) for n in range(2)], axis=1)

    def find_ends():
        for b in range(MID):
            x = nn(pick, both(1, b)).astype(BF16)
            for side in range(2):
                for n in range(2):
                    ends[side, b, n] = x[side * SIDE:(side + 1) * SIDE, n * e:(n + 1) * e]

    def find_outer():
        x = cat(nn(pick[SIDE:], both(0, last)), nn(pick[:SIDE], both(2, 0))).astype(BF16)
        for n in range(2):
            outer[n] = x[:, n * e:(n + 1) * e]

    lane = iota((1, 2 * SIDE), 1)

    def middle(m):
        q = qp[m].reshape(rows, e)
        kh, vh = kv[1, m, 0].reshape(rows, e), kv[1, m, 1].reshape(rows, e)
        mid = cat(*[nt(q[i * half:(i + 1) * half], kh[i * chunk:(i + 3) * chunk]) + mid_bias[i] for i in range(2)])
        top = jnp.maximum(jnp.max(mid[:, :e], axis=-1, keepdims=True), jnp.max(mid[:, e:], axis=-1, keepdims=True))
        p_mid = prob(mid, top)
        total = cat(*[nn(p_mid[i * half:(i + 1) * half], with_ones(vh[i * chunk:(i + 3) * chunk])) for i in range(2)])
        o_s[m] = total[:, :e]
        d_s[m] = total[:, e:]
        t_s[m] = jnp.broadcast_to(top, (rows, e))

    def near(b):
        q = qp[:, b].reshape(rows, e)
        kb, vb = kv[1, :, 0, b].reshape(rows, e), kv[1, :, 1, b].reshape(rows, e)
        k_rim, v_rim = (cat(ends[1, max(b - 1, 0), n], ends[0, min(b + 1, last), n]) for n in range(2))
        own = nt(q, kb) + near_bias[:, :rows]
        rim = nt(q, k_rim) + near_bias[:, rows:]
        if b == 0:
            rim += bias(lane >= SIDE)
        if b == last:
            rim += bias(lane < SIDE)
        at_b = pl.ds(b * chunk, chunk)
        old = t_s[:, at_b].reshape(rows, e)
        peak = jnp.maximum(jnp.maximum(own[:, :e], own[:, e:]), rim)
        top = jnp.maximum(old, jnp.max(peak, axis=-1, keepdims=True))
        fade = jnp.exp2((old - top) * SCALE)
        both = jnp.concatenate([top, top], axis=1)
        total = nn(prob(own, both), with_ones(vb)) + nn(prob(rim, top), with_ones(v_rim))
        o_s[:, at_b] = (fade * o_s[:, at_b].reshape(rows, e) + total[:, :e]).reshape(MID, chunk, e)
        d_s[:, at_b] = (fade * d_s[:, at_b].reshape(rows, e) + total[:, e:]).reshape(MID, chunk, e)
        t_s[:, at_b] = top.reshape(MID, chunk, e)

    def other_planes(m):
        q = qp[m].reshape(rows, e)
        k2 = [[kv[i, m, n].reshape(rows, e) for n in range(2)] for i in (0, 2, 1)]
        k_far, v_far = ([cat(*x) for x in zip(*(classes(k2[i][n]) for i in range(3)))] for n in range(2))
        far = [nt(a, b) for a, b in zip(classes(q), k_far)]
        near_far, own = unclass([x[:, :e] + far_bias[...] for x in far]), unclass([x[:, e:] for x in far])
        far = near_far
        k_rim, v_rim = (cat(k2[0][n][last * chunk:], k2[1][n][:chunk], outer[n]) for n in range(2))
        rim = nt(cat(q[:chunk], q[last * chunk:]), k_rim) + rim_bias[m]
        peak = jnp.maximum(rim[:, :e], rim[:, e:])
        peak = cat(jnp.maximum(far[:chunk], peak[:chunk]), far[chunk:last * chunk],
                   jnp.maximum(far[last * chunk:], peak[chunk:]))
        old = t_s[m]
        top = jnp.maximum(old, jnp.maximum(
            jnp.max(peak, axis=-1, keepdims=True), jnp.max(own, axis=-1, keepdims=True)))
        fade = jnp.exp2((old - top) * SCALE)
        p4 = jnp.concatenate([prob(far, top), prob(own, top[:, :chunk])], axis=1).reshape(MID, NS, mm, 3 * chunk)
        total = unclass([nn(p4[:, n].reshape(chunk, 3 * chunk), with_ones(v)) for n, v in enumerate(v_far)])
        top = cat(top[:chunk], top[last * chunk:])
        extra = nn(prob(rim, jnp.concatenate([top, top], axis=1)), with_ones(v_rim))
        total = cat(total[:chunk] + extra[:chunk], total[chunk:last * chunk], total[last * chunk:] + extra[chunk:])
        o = fade * o_s[m] + total[:, :e]
        den = fade * d_s[m] + total[:, e:]
        ob[m] = (o / den).astype(BF16).reshape(MID, chunk, e)

    def cols(core, head):
        return pl.ds(pl.multiple_of(core * width + head * e, e), e)

    def side(core):
        return pl.ds(pl.multiple_of(core * width, width), width)

    def result(m, d):
        return remote(ob.at[m, others[d]], att.at[m, :, cols(c, j)], res_s.at[0], res_r.at[m], mate(d), c)

    def across(m, b, to):
        return remote(ob.at[m, b], att.at[m, :, cols(c, j)], cross_s.at[0], cross_r.at[m - EARLY], to, 1 - c)

    def share(m):
        return remote(att.at[m, :, side(c)], att.at[m, :, side(c)], tp_s.at[0], tp_r.at[max(m - EARLY + 1, 0)], p, 1 - c)

    early = tuple(range(EARLY))
    late = tuple(range(EARLY, MID))

    def finish(ms):
        @pl.when(has_dn)
        def _():
            for m in ms:
                await_all(kv.at[0, m, :, pl.ds(0, last)], up_r.at[m])

        @pl.when(has_up)
        def _():
            for m in ms:
                await_all(kv.at[2, m, :, pl.ds(1, last)], dn_r.at[m])

        for m in ms:
            other_planes(m)
        for m in ms:
            for d in range(last):
                result(m, d).start()
            if m in late:
                @pl.when(c == 0)
                def _():
                    for d in range(last):
                        across(m, others[d], mate(d)).start()
                    across(m, j, p).start()
            att[m, :, cols(c, j)] = ob[m, pl.ds(j, 1)].reshape(chunk, e)

    def half_of(ms, core):
        x = att[ms[0]:ms[-1] + 1, :, side(core)].reshape(len(ms) * chunk, width)
        return nn(x, w_in[side(core), :])

    def begin(ms, core):
        partial[ms[0] * chunk:(ms[-1] + 1) * chunk] = half_of(ms, core)

    def complete(ms, y):
        for i, m in enumerate(ms):
            for n in range(NS):
                part = y[i * chunk + n * mm:i * chunk + (n + 1) * mm]
                for t in range(natural.shape[0]):
                    natural[t, pl.ds(MID * n + m, mm, stride=FAR), :] = part[:, t * e:(t + 1) * e]

    def end(ms, core):
        complete(ms, partial[ms[0] * chunk:(ms[-1] + 1) * chunk] + half_of(ms, core))

    for d in (1, 2, 0):
        b = others[d]
        await_all(kv.at[1, 0, :, b], give_r.at[b])

        @pl.when(has_up)
        def _():
            up(0, b).start()

        @pl.when(has_dn)
        def _():
            down(0, b).start()

    def arrival(m):
        await_all(kv.at[1, m, :, pl.ds(0, last)], give_r.at[last + m])

    arrival(1)
    for b in range(MID):
        relay(1, b, True, True)
    for m in range(2, MID):
        arrival(m)
        relay(m, last, True, False)
        relay(m, 0, False, True)
    for m in range(2, MID):
        for b in range(MID):
            relay(m, b, b != last, b != 0)
    find_ends()
    await_all(qp.at[pl.ds(0, 2), pl.ds(0, last)], ask_r.at[0])
    middle(0)
    middle(1)
    await_all(qp.at[pl.ds(0, 2), pl.ds(0, last)], ask_r.at[1])
    middle(2)
    middle(3)
    for b in range(MID):
        near(b)
    @pl.when(has_dn)
    def _():
        await_all(kv.at[0, :, :, last], up_r.at[MID])

    @pl.when(has_up)
    def _():
        await_all(kv.at[2, :, :, 0], dn_r.at[MID])

    find_outer()
    finish((0, 1))
    finish((2,))
    finish((3,))
    for m in early:
        await_all(ob.at[m, pl.ds(0, last)], res_r.at[m])
        share(m).start()
    loads[3].wait()
    @pl.when(c == 0)
    def _():
        begin(early, 0)
        await_all(att.at[pl.ds(0, EARLY), :, side(1)], tp_r.at[0])
        end(early, 1)
        for m in late:
            await_all(att.at[m, :, side(1)], tp_r.at[m - EARLY + 1])
        begin(late, 1)
        for m in late:
            await_all(ob.at[m, pl.ds(0, last)], res_r.at[m])
            end((m,), 0)

    @pl.when(c == 1)
    def _():
        for m in late:
            await_all(ob.at[m, pl.ds(0, last)], res_r.at[m])
            share(m).start()
        begin(tuple(range(MID)), 1)
        await_all(ob.at[late[0]], cross_r.at[0])
        end(late[:1], 0)
        await_all(att.at[pl.ds(0, EARLY), :, side(0)], tp_r.at[0])
        end(early, 0)
        for m in late[1:]:
            await_all(ob.at[m], cross_r.at[m - EARLY])
            end((m,), 0)

    for t in range(natural.shape[0]):
        out_ref[:, t * e:(t + 1) * e] = natural[t].astype(BF16)

    await_all(ps.at[:, pl.ds(0, last), pair], give_s.at[0])
    await_all(ps.at[:, pl.ds(0, last), 2], ask_s.at[0])
    await_all(ob.at[:, pl.ds(0, last)], res_s.at[0])

    @pl.when(c == 0)
    def _():
        await_all(ob.at[pl.ds(0, MID - EARLY)], cross_s.at[0])
        await_all(att.at[pl.ds(0, EARLY), :, side(c)], tp_s.at[0])

    @pl.when(c == 1)
    def _():
        await_all(att.at[:, :, side(c)], tp_s.at[0])

    @pl.when(has_up)
    def _():
        await_all(kv.at[0], up_s.at[0])

    @pl.when(has_dn)
    def _():
        await_all(kv.at[2], dn_s.at[0])


def per_device(sp_n, q, k, v, w):
    rows, columns = q.shape
    heads = columns // HEAD_DIM
    assert MID * rows == SIDE * FAR and rows // MID == SIDE and sp_n % MID == 0 and heads == MID
    dma = pltpu.SemaphoreType.DMA
    e, chunk = HEAD_DIM, rows // MID
    vmem = lambda *shape, dtype=BF16: pltpu.VMEM(shape, dtype)
    pinned = [pltpu.with_memory_space_constraint(x, pltpu.HBM) for x in (q, k, v, w)]
    return pl.pallas_call(
        functools.partial(kernel, sp_n, heads),
        out_shape=pltpu.VMEM((rows, w.shape[1]), BF16),
        in_specs=[pl.BlockSpec(memory_space=pltpu.HBM)] * 4,
        out_specs=pl.BlockSpec(memory_space=pltpu.VMEM),
        scratch_shapes=[
            vmem(rows, columns), vmem(rows, columns), vmem(rows, columns), vmem(*w.shape),
            vmem(MID, heads, 3, chunk, e),
            vmem(3, MID, 2, MID, chunk, e),
            vmem(MID, MID, chunk, e),
            vmem(2, MID, 2, SIDE, e),
            vmem(2, 2 * SIDE, e),
            vmem(rows, rows + 2 * SIDE, dtype=F32),
            vmem(2, rows // 2, 3 * chunk, dtype=F32),
            vmem(chunk, 2 * chunk, dtype=F32),
            vmem(MID, rows // 2, 4 * chunk, dtype=F32),
            vmem(MID, rows, e, dtype=F32), vmem(MID, rows, e, dtype=F32), vmem(MID, rows, e, dtype=F32),
            vmem(MID, MID, chunk, e),
            vmem(MID, chunk, 2 * columns),
            vmem(rows, w.shape[1], dtype=F32),
            vmem(w.shape[1] // e, rows, e, dtype=F32),
            dma((4,)),
            dma((1,)), dma((2 * MID - 1,)),
            dma((1,)), dma((2,)),
            dma((1,)), dma((MID + 1,)),
            dma((1,)), dma((MID + 1,)),
            dma((1,)), dma((MID,)),
            dma((1,)), dma((MID - EARLY,)),
            dma((1,)), dma((MID - EARLY + 1,)),
        ],
        compiler_params=pltpu.CompilerParams(
            collective_id=0, has_side_effects=True, vmem_limit_bytes=40 * 1024 * 1024),
    )(*pinned)


def solution(mesh):
    return jax.shard_map(
        functools.partial(per_device, mesh.shape["sp"]), mesh=mesh,
        in_specs=(P("sp", "tp"), P("sp", "tp"), P("sp", "tp"), P(None, "tp")),
        out_specs=P("sp", "tp"), check_vma=False,
    )
```

```python
import functools
import math

import jax
import jax.numpy as jnp
from jax import lax
from jax.experimental import pallas as pl
from jax.experimental.pallas import tpu as pltpu
from jax.sharding import PartitionSpec as P

HEAD_DIM = 128
SIDE = 64
MID = 4
FAR = 16
NS = FAR // MID
MESH = pl.DeviceIdType.MESH
F32 = jnp.float32
BF16 = jnp.bfloat16
SCALE = HEAD_DIM ** -0.5 * math.log2(math.e)
NEG = -jnp.inf
EARLY = 2


def nt(a, b):
    return lax.dot_general(a, b, (((1,), (1,)), ((), ())), preferred_element_type=F32)


def nn(a, b):
    return lax.dot_general(a, b, (((1,), (0,)), ((), ())), preferred_element_type=F32)


def iota(shape, dim):
    return lax.broadcasted_iota(jnp.int32, shape, dim)


def bias(ok):
    return jnp.where(ok, 0.0, NEG).astype(F32)


def kernel(sp_n, heads, q_hbm, k_hbm, v_hbm, w_hbm, out_ref,
           q_in, k_in, v_in, w_in, ps, kv, qp, ends, outer, near_bias, mid_bias, far_bias, rim_bias,
           o_s, t_s, d_s, ob, att, partial, natural,
           load_sem, give_s, give_r, ask_s, ask_r, up_s, up_r, dn_s, dn_r, res_s, res_r, cross_s, cross_r, tp_s, tp_r):
    rows = q_in.shape[0]
    chunk = rows // MID
    mm = rows // FAR
    e = HEAD_DIM
    width = heads * e
    last = MID - 1
    p, c = lax.axis_index("sp"), lax.axis_index("tp")
    groups = sp_n // MID
    g, j = p // MID, p % MID

    loads = [
        pltpu.make_async_copy(src, dst, load_sem.at[n])
        for n, (src, dst) in enumerate(((k_hbm, k_in), (v_hbm, v_in), (q_hbm, q_in), (w_hbm, w_in)))
    ]
    for load in loads[:3]:
        load.start()

    barrier = pltpu.get_barrier_semaphore()

    def greet(sp, tp):
        pl.semaphore_signal(barrier, inc=1, device_id=(sp, tp), device_id_type=MESH)

    others = (MID - 1 - j, j + 1 - 2 * (j % 2), (j + MID // 2) % MID)

    def mate(d):
        return g * MID + others[d]

    for d in range(last):
        greet(mate(d), c)
        greet(mate(d), 1 - c)
    greet(p, 1 - c)
    has_dn, has_up = g > 0, g < groups - 1
    up_p, dn_p = (p + MID) % sp_n, (p - MID + sp_n) % sp_n

    @pl.when(has_dn)
    def _():
        greet(dn_p, c)

    @pl.when(has_up)
    def _():
        greet(up_p, c)

    def remote(src, dst, ss, rs, sp, tp):
        return pltpu.make_async_remote_copy(
            src_ref=src, dst_ref=dst, send_sem=ss, recv_sem=rs, device_id=(sp, tp), device_id_type=MESH)

    def await_all(ref, sem):
        pltpu.make_async_copy(ref, ref, sem).wait()

    def token(r):
        return FAR * (r % mm) + MID * ((r % chunk) // mm) + r // chunk

    r, t = iota((rows, rows), 0), iota((rows, rows), 1)
    perm = (t == token(r)).astype(BF16)

    def reorder(*arrays):
        for n, _ in arrays:
            loads[n].wait()
        for n, x in arrays:
            moved = nn(perm, x[...]).astype(BF16)
            for h in range(heads):
                for m in range(MID):
                    ps[m, h, n] = moved[m * chunk:(m + 1) * chunk, h * e:(h + 1) * e]

    reorder((0, k_in), (1, v_in))

    @pl.when(jnp.logical_not(has_dn))
    def _():
        kv[0] = jnp.zeros(kv.shape[1:], BF16)

    @pl.when(jnp.logical_not(has_up))
    def _():
        kv[2] = jnp.zeros(kv.shape[1:], BF16)

    pl.semaphore_wait(barrier, 2 * MID - 1 + has_dn.astype(jnp.int32) + has_up.astype(jnp.int32))

    pair = pl.ds(0, 2)

    def give(m, d):
        return remote(ps.at[m, others[d], pair], kv.at[1, m, :, j], give_s.at[0], give_r.at[j if m == 0 else last + m], mate(d), c)

    def ask(i, d):
        two = pl.ds(2 * i, 2)
        return remote(ps.at[two, others[d], 2], qp.at[two, j], ask_s.at[0], ask_r.at[i], mate(d), c)

    def up(m, b, own=False):
        src = ps.at[m, j, pair] if own else kv.at[1, m, :, b]
        edge = (b == last).astype(jnp.int32) if hasattr(b, "astype") else int(b == last)
        arrived = edge * MID + (1 - edge) * m
        return remote(src, kv.at[0, m, :, b], up_s.at[0], up_r.at[arrived], up_p, c)

    def down(m, b, own=False):
        src = ps.at[m, j, pair] if own else kv.at[1, m, :, b]
        edge = (b == 0).astype(jnp.int32) if hasattr(b, "astype") else int(b == 0)
        arrived = edge * MID + (1 - edge) * m
        return remote(src, kv.at[2, m, :, b], dn_s.at[0], dn_r.at[arrived], dn_p, c)

    for m in range(MID):
        for d in ((1, 2, 0) if m == 0 else range(last)):
            give(m, d).start()
        if m == 0:
            @pl.when(has_up)
            def _():
                for i in range(MID):
                    up(i, j, own=True).start()

            @pl.when(has_dn)
            def _():
                for i in range(MID):
                    down(i, j, own=True).start()

    reorder((2, q_in))
    for i in range(2):
        for d in range(last):
            ask(i, d).start()

    loads[3].start()
    for m in range(MID):
        kv[1, m, :, pl.ds(j, 1)] = ps[m, pl.ds(j, 1), 0:2].reshape(2, 1, chunk, e)
        qp[m, pl.ds(j, 1)] = ps[m, pl.ds(j, 1), 2]

    ok_dn, ok_up = has_dn.astype(jnp.int32) == 1, has_up.astype(jnp.int32) == 1
    tq, s = token(iota((rows, rows), 0)), iota((rows, rows), 1)
    gap = tq - token(s)
    near_bias[:, :rows] = bias((gap >= -SIDE) & (gap <= SIDE))
    tq, s = token(iota((rows, 2 * SIDE), 0)), iota((rows, 2 * SIDE), 1)
    near_bias[:, rows:] = bias(((s < SIDE) & (s >= tq)) | ((s >= SIDE) & (s - SIDE <= tq - (rows - SIDE))))

    def order(x):
        return chunk * (x // chunk) + NS * (x % mm) + (x % chunk) // mm

    half = rows // 2
    uq, uk = order(iota((half, 3 * chunk), 0)), order(iota((half, 3 * chunk), 1))
    for i in range(2):
        gap = uk - uq - i * chunk
        mid_bias[i] = bias((gap >= -SIDE) & (gap <= SIDE))
    x, s = iota((chunk, 2 * chunk), 0), iota((chunk, 2 * chunk), 1)
    far_bias[...] = bias(((s < chunk) & (s >= x) & ok_dn) | ((s >= chunk) & (s - chunk <= x) & ok_up))
    x, s = iota((half, 2 * chunk), 0), iota((half, 2 * chunk), 1)
    u, v = order(x % chunk), order(s % chunk)
    low, high = (x < chunk) & (s < chunk) & ok_dn, (x >= chunk) & (s >= chunk) & ok_up
    for m in range(MID):
        tq = token(m * chunk + x % chunk)
        rim_bias[m, :, :2 * chunk] = bias((low & (v >= u)) | (high & (v <= u)))
        rim_bias[m, :, 2 * chunk:] = bias((low & (s >= tq)) | (high & (s - SIDE <= tq - (rows - SIDE))))

    def relay(m, b, rise, fall):
        if rise:
            @pl.when((j != b) & has_up)
            def _():
                up(m, b).start()

        if fall:
            @pl.when((j != b) & has_dn)
            def _():
                down(m, b).start()

    def classes(x):
        x4 = x.reshape(MID, NS, mm, e)
        return [x4[:, n].reshape(chunk, e) for n in range(NS)]

    def unclass(parts):
        return jnp.concatenate([parts[n][i * mm:(i + 1) * mm] for i in range(MID) for n in range(NS)], axis=0)

    def cat(*parts):
        return jnp.concatenate(parts, axis=0)

    def with_ones(x):
        return jnp.concatenate([x, jnp.ones((x.shape[0], e), BF16)], axis=1)

    def prob(s, top):
        return jnp.exp2((s - top) * SCALE).astype(BF16)

    x, s = iota((2 * SIDE, rows), 0), iota((2 * SIDE, rows), 1)
    pick = (token(s) == x + (x // SIDE) * (rows - 2 * SIDE)).astype(BF16)

    def both(i, b):
        return jnp.concatenate([kv[i, :, n, b].reshape(rows, e) for n in range(2)], axis=1)

    def find_ends():
        for b in range(MID):
            x = nn(pick, both(1, b)).astype(BF16)
            for side in range(2):
                for n in range(2):
                    ends[side, b, n] = x[side * SIDE:(side + 1) * SIDE, n * e:(n + 1) * e]

    def find_outer():
        x = cat(nn(pick[SIDE:], both(0, last)), nn(pick[:SIDE], both(2, 0))).astype(BF16)
        for n in range(2):
            outer[n] = x[:, n * e:(n + 1) * e]

    lane = iota((1, 2 * SIDE), 1)

    def middle(m):
        q = qp[m].reshape(rows, e)
        kh, vh = kv[1, m, 0].reshape(rows, e), kv[1, m, 1].reshape(rows, e)
        mid = cat(*[nt(q[i * half:(i + 1) * half], kh[i * chunk:(i + 3) * chunk]) + mid_bias[i] for i in range(2)])
        top = jnp.maximum(jnp.max(mid[:, :e], axis=-1, keepdims=True), jnp.max(mid[:, e:], axis=-1, keepdims=True))
        p_mid = prob(mid, top)
        total = cat(*[nn(p_mid[i * half:(i + 1) * half], with_ones(vh[i * chunk:(i + 3) * chunk])) for i in range(2)])
        o_s[m] = total[:, :e]
        d_s[m] = total[:, e:]
        t_s[m] = jnp.broadcast_to(top, (rows, e))

    def rims(b, n):
        return cat(ends[1, max(b - 1, 0), n], ends[0, min(b + 1, last), n])

    def near_scores(b):
        q = qp[:, b].reshape(rows, e)
        k_rim = rims(b, 0)
        own = nt(q, kv[1, :, 0, b].reshape(rows, e)) + near_bias[:, :rows]
        rim = nt(q, k_rim) + near_bias[:, rows:]
        if b == 0:
            rim += bias(lane >= SIDE)
        if b == last:
            rim += bias(lane < SIDE)
        return own, rim

    def near(b, own, rim):
        vb, v_rim = kv[1, :, 1, b].reshape(rows, e), rims(b, 1)
        at_b = pl.ds(b * chunk, chunk)
        old = t_s[:, at_b].reshape(rows, e)
        peak = jnp.maximum(jnp.maximum(own[:, :e], own[:, e:]), rim)
        top = jnp.maximum(old, jnp.max(peak, axis=-1, keepdims=True))
        fade = jnp.exp2((old - top) * SCALE)
        both = jnp.concatenate([top, top], axis=1)
        total = nn(prob(own, both), with_ones(vb)) + nn(prob(rim, top), with_ones(v_rim))
        o_s[:, at_b] = (fade * o_s[:, at_b].reshape(rows, e) + total[:, :e]).reshape(MID, chunk, e)
        d_s[:, at_b] = (fade * d_s[:, at_b].reshape(rows, e) + total[:, e:]).reshape(MID, chunk, e)
        t_s[:, at_b] = top.reshape(MID, chunk, e)

    def other_planes(m):
        q = qp[m].reshape(rows, e)
        k2 = [[kv[i, m, n].reshape(rows, e) for n in range(2)] for i in (0, 2, 1)]
        k_far, v_far = ([cat(*x) for x in zip(*(classes(k2[i][n]) for i in range(3)))] for n in range(2))
        far = [nt(a, b) for a, b in zip(classes(q), k_far)]
        near_far, own = unclass([x[:, :e] + far_bias[...] for x in far]), unclass([x[:, e:] for x in far])
        far = near_far
        k_rim, v_rim = (cat(k2[0][n][last * chunk:], k2[1][n][:chunk], outer[n]) for n in range(2))
        rim = nt(cat(q[:chunk], q[last * chunk:]), k_rim) + rim_bias[m]
        peak = jnp.maximum(rim[:, :e], rim[:, e:])
        peak = cat(jnp.maximum(far[:chunk], peak[:chunk]), far[chunk:last * chunk],
                   jnp.maximum(far[last * chunk:], peak[chunk:]))
        old = t_s[m]
        top = jnp.maximum(old, jnp.maximum(
            jnp.max(peak, axis=-1, keepdims=True), jnp.max(own, axis=-1, keepdims=True)))
        fade = jnp.exp2((old - top) * SCALE)
        p4 = jnp.concatenate([prob(far, top), prob(own, top[:, :chunk])], axis=1).reshape(MID, NS, mm, 3 * chunk)
        total = unclass([nn(p4[:, n].reshape(chunk, 3 * chunk), with_ones(v)) for n, v in enumerate(v_far)])
        top = cat(top[:chunk], top[last * chunk:])
        extra = nn(prob(rim, jnp.concatenate([top, top], axis=1)), with_ones(v_rim))
        total = cat(total[:chunk] + extra[:chunk], total[chunk:last * chunk], total[last * chunk:] + extra[chunk:])
        o = fade * o_s[m] + total[:, :e]
        den = fade * d_s[m] + total[:, e:]
        ob[m] = (o / den).astype(BF16).reshape(MID, chunk, e)

    def cols(core, head):
        return pl.ds(pl.multiple_of(core * width + head * e, e), e)

    def side(core):
        return pl.ds(pl.multiple_of(core * width, width), width)

    def result(m, d):
        return remote(ob.at[m, others[d]], att.at[m, :, cols(c, j)], res_s.at[0], res_r.at[m], mate(d), c)

    def across(m, b, to):
        return remote(ob.at[m, b], att.at[m, :, cols(c, j)], cross_s.at[0], cross_r.at[m - EARLY], to, 1 - c)

    def share(m):
        return remote(att.at[m, :, side(c)], att.at[m, :, side(c)], tp_s.at[0], tp_r.at[max(m - EARLY + 1, 0)], p, 1 - c)

    early = tuple(range(EARLY))
    late = tuple(range(EARLY, MID))

    def finish(ms):
        @pl.when(has_dn)
        def _():
            for m in ms:
                await_all(kv.at[0, m, :, pl.ds(0, last)], up_r.at[m])

        @pl.when(has_up)
        def _():
            for m in ms:
                await_all(kv.at[2, m, :, pl.ds(1, last)], dn_r.at[m])

        if ms[0] == 0:
            find_outer()
        for m in ms:
            other_planes(m)
        for m in ms:
            for d in range(last):
                result(m, d).start()
            if m in late:
                @pl.when(c == 0)
                def _():
                    for d in range(last):
                        across(m, others[d], mate(d)).start()
                    across(m, j, p).start()
            att[m, :, cols(c, j)] = ob[m, pl.ds(j, 1)].reshape(chunk, e)

    def half_of(ms, core):
        x = att[ms[0]:ms[-1] + 1, :, side(core)].reshape(len(ms) * chunk, width)
        return nn(x, w_in[side(core), :])

    def begin(ms, core):
        partial[ms[0] * chunk:(ms[-1] + 1) * chunk] = half_of(ms, core)

    def complete(ms, y):
        for i, m in enumerate(ms):
            for n in range(NS):
                part = y[i * chunk + n * mm:i * chunk + (n + 1) * mm]
                for t in range(natural.shape[0]):
                    natural[t, pl.ds(MID * n + m, mm, stride=FAR), :] = part[:, t * e:(t + 1) * e]

    def end(ms, core):
        complete(ms, partial[ms[0] * chunk:(ms[-1] + 1) * chunk] + half_of(ms, core))

    for d in (1, 2, 0):
        b = others[d]
        await_all(kv.at[1, 0, :, b], give_r.at[b])

        @pl.when(has_up)
        def _():
            up(0, b).start()

        @pl.when(has_dn)
        def _():
            down(0, b).start()

    def arrival(m):
        await_all(kv.at[1, m, :, pl.ds(0, last)], give_r.at[last + m])

    arrival(1)
    for b in range(MID):
        relay(1, b, True, True)
    for m in range(2, MID):
        arrival(m)
        relay(m, last, True, False)
        relay(m, 0, False, True)
    for m in range(2, MID):
        for b in range(MID):
            relay(m, b, b != last, b != 0)
    find_ends()
    await_all(qp.at[pl.ds(0, 2), pl.ds(0, last)], ask_r.at[0])
    middle(0)
    middle(1)
    await_all(qp.at[pl.ds(0, 2), pl.ds(0, last)], ask_r.at[1])
    middle(2)
    scores = near_scores(0)
    middle(3)
    for b in range(MID):
        now, scores = scores, near_scores(b + 1) if b < last else None
        near(b, *now)
    @pl.when(has_dn)
    def _():
        await_all(kv.at[0, :, :, last], up_r.at[MID])

    @pl.when(has_up)
    def _():
        await_all(kv.at[2, :, :, 0], dn_r.at[MID])

    finish((0, 1))
    finish((2,))
    finish((3,))
    for m in early:
        await_all(ob.at[m, pl.ds(0, last)], res_r.at[m])
        share(m).start()
    loads[3].wait()
    @pl.when(c == 0)
    def _():
        begin(early, 0)
        await_all(att.at[pl.ds(0, EARLY), :, side(1)], tp_r.at[0])
        end(early, 1)
        for m in late:
            await_all(att.at[m, :, side(1)], tp_r.at[m - EARLY + 1])
        begin(late, 1)
        for m in late:
            await_all(ob.at[m, pl.ds(0, last)], res_r.at[m])
            end((m,), 0)

    @pl.when(c == 1)
    def _():
        for m in late:
            await_all(ob.at[m, pl.ds(0, last)], res_r.at[m])
            share(m).start()
        begin(tuple(range(MID)), 1)
        await_all(ob.at[late[0]], cross_r.at[0])
        end(late[:1], 0)
        await_all(att.at[pl.ds(0, EARLY), :, side(0)], tp_r.at[0])
        end(early, 0)
        for m in late[1:]:
            await_all(ob.at[m], cross_r.at[m - EARLY])
            end((m,), 0)

    for t in range(natural.shape[0]):
        out_ref[:, t * e:(t + 1) * e] = natural[t].astype(BF16)

    await_all(ps.at[:, pl.ds(0, last), pair], give_s.at[0])
    await_all(ps.at[:, pl.ds(0, last), 2], ask_s.at[0])
    await_all(ob.at[:, pl.ds(0, last)], res_s.at[0])

    @pl.when(c == 0)
    def _():
        await_all(ob.at[pl.ds(0, MID - EARLY)], cross_s.at[0])
        await_all(att.at[pl.ds(0, EARLY), :, side(c)], tp_s.at[0])

    @pl.when(c == 1)
    def _():
        await_all(att.at[:, :, side(c)], tp_s.at[0])

    @pl.when(has_up)
    def _():
        await_all(kv.at[0], up_s.at[0])

    @pl.when(has_dn)
    def _():
        await_all(kv.at[2], dn_s.at[0])


def per_device(sp_n, q, k, v, w):
    rows, columns = q.shape
    heads = columns // HEAD_DIM
    assert MID * rows == SIDE * FAR and rows // MID == SIDE and sp_n % MID == 0 and heads == MID
    dma = pltpu.SemaphoreType.DMA
    e, chunk = HEAD_DIM, rows // MID
    vmem = lambda *shape, dtype=BF16: pltpu.VMEM(shape, dtype)
    pinned = [pltpu.with_memory_space_constraint(x, pltpu.HBM) for x in (q, k, v, w)]
    return pl.pallas_call(
        functools.partial(kernel, sp_n, heads),
        out_shape=pltpu.VMEM((rows, w.shape[1]), BF16),
        in_specs=[pl.BlockSpec(memory_space=pltpu.HBM)] * 4,
        out_specs=pl.BlockSpec(memory_space=pltpu.VMEM),
        scratch_shapes=[
            vmem(rows, columns), vmem(rows, columns), vmem(rows, columns), vmem(*w.shape),
            vmem(MID, heads, 3, chunk, e),
            vmem(3, MID, 2, MID, chunk, e),
            vmem(MID, MID, chunk, e),
            vmem(2, MID, 2, SIDE, e),
            vmem(2, 2 * SIDE, e),
            vmem(rows, rows + 2 * SIDE, dtype=F32),
            vmem(2, rows // 2, 3 * chunk, dtype=F32),
            vmem(chunk, 2 * chunk, dtype=F32),
            vmem(MID, rows // 2, 4 * chunk, dtype=F32),
            vmem(MID, rows, e, dtype=F32), vmem(MID, rows, e, dtype=F32), vmem(MID, rows, e, dtype=F32),
            vmem(MID, MID, chunk, e),
            vmem(MID, chunk, 2 * columns),
            vmem(rows, w.shape[1], dtype=F32),
            vmem(w.shape[1] // e, rows, e, dtype=F32),
            dma((4,)),
            dma((1,)), dma((2 * MID - 1,)),
            dma((1,)), dma((2,)),
            dma((1,)), dma((MID + 1,)),
            dma((1,)), dma((MID + 1,)),
            dma((1,)), dma((MID,)),
            dma((1,)), dma((MID - EARLY,)),
            dma((1,)), dma((MID - EARLY + 1,)),
        ],
        compiler_params=pltpu.CompilerParams(
            collective_id=0, has_side_effects=True, vmem_limit_bytes=40 * 1024 * 1024),
    )(*pinned)


def solution(mesh):
    return jax.shard_map(
        functools.partial(per_device, mesh.shape["sp"]), mesh=mesh,
        in_specs=(P("sp", "tp"), P("sp", "tp"), P("sp", "tp"), P(None, "tp")),
        out_specs=P("sp", "tp"), check_vma=False,
    )
```

```python
import functools
import math

import jax
import jax.numpy as jnp
from jax import lax
from jax.experimental import pallas as pl
from jax.experimental.pallas import tpu as pltpu
from jax.sharding import PartitionSpec as P

HEAD_DIM = 128
SIDE = 64
MID = 4
FAR = 16
NS = FAR // MID
MESH = pl.DeviceIdType.MESH
F32 = jnp.float32
BF16 = jnp.bfloat16
SCALE = HEAD_DIM ** -0.5 * math.log2(math.e)
NEG = -jnp.inf
EARLY = 2


def nt(a, b):
    return lax.dot_general(a, b, (((1,), (1,)), ((), ())), preferred_element_type=F32)


def nn(a, b):
    return lax.dot_general(a, b, (((1,), (0,)), ((), ())), preferred_element_type=F32)


def iota(shape, dim):
    return lax.broadcasted_iota(jnp.int32, shape, dim)


def bias(ok):
    return jnp.where(ok, 0.0, NEG).astype(F32)


def kernel(sp_n, heads, q_hbm, k_hbm, v_hbm, w_hbm, out_ref,
           q_in, k_in, v_in, w_in, ps, kv, qp, ends, outer, near_bias, mid_bias, far_bias, rim_bias,
           o_s, t_s, d_s, ob, att, partial, natural,
           load_sem, give_s, give_r, ask_s, ask_r, up_s, up_r, dn_s, dn_r, res_s, res_r, cross_s, cross_r, tp_s, tp_r):
    rows = q_in.shape[0]
    chunk = rows // MID
    mm = rows // FAR
    e = HEAD_DIM
    width = heads * e
    last = MID - 1
    p, c = lax.axis_index("sp"), lax.axis_index("tp")
    groups = sp_n // MID
    g, j = p // MID, p % MID

    loads = [
        pltpu.make_async_copy(src, dst, load_sem.at[n])
        for n, (src, dst) in enumerate(((k_hbm, k_in), (v_hbm, v_in), (q_hbm, q_in), (w_hbm, w_in)))
    ]
    for load in loads[:3]:
        load.start()

    barrier = pltpu.get_barrier_semaphore()

    def greet(sp, tp):
        pl.semaphore_signal(barrier, inc=1, device_id=(sp, tp), device_id_type=MESH)

    others = (MID - 1 - j, j + 1 - 2 * (j % 2), (j + MID // 2) % MID)

    def mate(d):
        return g * MID + others[d]

    for d in range(last):
        greet(mate(d), c)
        greet(mate(d), 1 - c)
    greet(p, 1 - c)
    has_dn, has_up = g > 0, g < groups - 1
    up_p, dn_p = (p + MID) % sp_n, (p - MID + sp_n) % sp_n

    @pl.when(has_dn)
    def _():
        greet(dn_p, c)

    @pl.when(has_up)
    def _():
        greet(up_p, c)

    def remote(src, dst, ss, rs, sp, tp):
        return pltpu.make_async_remote_copy(
            src_ref=src, dst_ref=dst, send_sem=ss, recv_sem=rs, device_id=(sp, tp), device_id_type=MESH)

    def await_all(ref, sem):
        pltpu.make_async_copy(ref, ref, sem).wait()

    def token(r):
        return FAR * (r % mm) + MID * ((r % chunk) // mm) + r // chunk

    r, t = iota((rows, rows), 0), iota((rows, rows), 1)
    perm = (t == token(r)).astype(BF16)

    def reorder(*arrays):
        for n, _ in arrays:
            loads[n].wait()
        for n, x in arrays:
            moved = nn(perm, x[...]).astype(BF16)
            for h in range(heads):
                for m in range(MID):
                    ps[m, h, n] = moved[m * chunk:(m + 1) * chunk, h * e:(h + 1) * e]

    reorder((0, k_in), (1, v_in))

    @pl.when(jnp.logical_not(has_dn))
    def _():
        kv[0] = jnp.zeros(kv.shape[1:], BF16)

    @pl.when(jnp.logical_not(has_up))
    def _():
        kv[2] = jnp.zeros(kv.shape[1:], BF16)

    pl.semaphore_wait(barrier, 2 * MID - 1 + has_dn.astype(jnp.int32) + has_up.astype(jnp.int32))

    pair = pl.ds(0, 2)

    def give(m, d):
        return remote(ps.at[m, others[d], pair], kv.at[1, m, :, j], give_s.at[0], give_r.at[j if m == 0 else last + m], mate(d), c)

    def ask(i, d):
        two = pl.ds(2 * i, 2)
        return remote(ps.at[two, others[d], 2], qp.at[two, j], ask_s.at[0], ask_r.at[i], mate(d), c)

    def up(m, b, own=False):
        src = ps.at[m, j, pair] if own else kv.at[1, m, :, b]
        edge = (b == last).astype(jnp.int32) if hasattr(b, "astype") else int(b == last)
        arrived = edge * MID + (1 - edge) * m
        return remote(src, kv.at[0, m, :, b], up_s.at[0], up_r.at[arrived], up_p, c)

    def down(m, b, own=False):
        src = ps.at[m, j, pair] if own else kv.at[1, m, :, b]
        edge = (b == 0).astype(jnp.int32) if hasattr(b, "astype") else int(b == 0)
        arrived = edge * MID + (1 - edge) * m
        return remote(src, kv.at[2, m, :, b], dn_s.at[0], dn_r.at[arrived], dn_p, c)

    for m in range(MID):
        for d in ((1, 2, 0) if m == 0 else range(last)):
            give(m, d).start()
        if m == 0:
            @pl.when(has_up)
            def _():
                for i in range(MID):
                    up(i, j, own=True).start()

            @pl.when(has_dn)
            def _():
                for i in range(MID):
                    down(i, j, own=True).start()

    reorder((2, q_in))
    for i in range(2):
        for d in range(last):
            ask(i, d).start()

    loads[3].start()
    for m in range(MID):
        kv[1, m, :, pl.ds(j, 1)] = ps[m, pl.ds(j, 1), 0:2].reshape(2, 1, chunk, e)
        qp[m, pl.ds(j, 1)] = ps[m, pl.ds(j, 1), 2]

    ok_dn, ok_up = has_dn.astype(jnp.int32) == 1, has_up.astype(jnp.int32) == 1
    tq, s = token(iota((rows, rows), 0)), iota((rows, rows), 1)
    gap = tq - token(s)
    near_bias[:, :rows] = bias((gap >= -SIDE) & (gap <= SIDE))
    tq, s = token(iota((rows, 2 * SIDE), 0)), iota((rows, 2 * SIDE), 1)
    near_bias[:, rows:] = bias(((s < SIDE) & (s >= tq)) | ((s >= SIDE) & (s - SIDE <= tq - (rows - SIDE))))

    def order(x):
        return chunk * (x // chunk) + NS * (x % mm) + (x % chunk) // mm

    half = rows // 2
    uq, uk = order(iota((half, 3 * chunk), 0)), order(iota((half, 3 * chunk), 1))
    for i in range(2):
        gap = uk - uq - i * chunk
        mid_bias[i] = bias((gap >= -SIDE) & (gap <= SIDE))
    x, s = iota((chunk, 2 * chunk), 0), iota((chunk, 2 * chunk), 1)
    far_bias[...] = bias(((s < chunk) & (s >= x) & ok_dn) | ((s >= chunk) & (s - chunk <= x) & ok_up))
    x, s = iota((half, 2 * chunk), 0), iota((half, 2 * chunk), 1)
    u, v = order(x % chunk), order(s % chunk)
    low, high = (x < chunk) & (s < chunk) & ok_dn, (x >= chunk) & (s >= chunk) & ok_up
    for m in range(MID):
        tq = token(m * chunk + x % chunk)
        rim_bias[m, :, :2 * chunk] = bias((low & (v >= u)) | (high & (v <= u)))
        rim_bias[m, :, 2 * chunk:] = bias((low & (s >= tq)) | (high & (s - SIDE <= tq - (rows - SIDE))))

    def relay(m, b, rise, fall):
        if rise:
            @pl.when((j != b) & has_up)
            def _():
                up(m, b).start()

        if fall:
            @pl.when((j != b) & has_dn)
            def _():
                down(m, b).start()

    def classes(x):
        x4 = x.reshape(MID, NS, mm, e)
        return [x4[:, n].reshape(chunk, e) for n in range(NS)]

    def unclass(parts):
        return jnp.concatenate([parts[n][i * mm:(i + 1) * mm] for i in range(MID) for n in range(NS)], axis=0)

    def cat(*parts):
        return jnp.concatenate(parts, axis=0)

    def with_ones(x):
        return jnp.concatenate([x, jnp.ones((x.shape[0], e), BF16)], axis=1)

    def prob(s, top):
        return jnp.exp2((s - top) * SCALE).astype(BF16)

    x, s = iota((2 * SIDE, rows), 0), iota((2 * SIDE, rows), 1)
    pick = (token(s) == x + (x // SIDE) * (rows - 2 * SIDE)).astype(BF16)

    def both(i, b):
        return jnp.concatenate([kv[i, :, n, b].reshape(rows, e) for n in range(2)], axis=1)

    def find_ends():
        for b in range(MID):
            x = nn(pick, both(1, b)).astype(BF16)
            for side in range(2):
                for n in range(2):
                    ends[side, b, n] = x[side * SIDE:(side + 1) * SIDE, n * e:(n + 1) * e]

    def find_outer():
        x = cat(nn(pick[SIDE:], both(0, last)), nn(pick[:SIDE], both(2, 0))).astype(BF16)
        for n in range(2):
            outer[n] = x[:, n * e:(n + 1) * e]

    lane = iota((1, 2 * SIDE), 1)

    def middle(m):
        q = qp[m].reshape(rows, e)
        kh, vh = kv[1, m, 0].reshape(rows, e), kv[1, m, 1].reshape(rows, e)
        mid = cat(*[nt(q[i * half:(i + 1) * half], kh[i * chunk:(i + 3) * chunk]) + mid_bias[i] for i in range(2)])
        top = jnp.maximum(jnp.max(mid[:, :e], axis=-1, keepdims=True), jnp.max(mid[:, e:], axis=-1, keepdims=True))
        p_mid = prob(mid, top)
        total = cat(*[nn(p_mid[i * half:(i + 1) * half], with_ones(vh[i * chunk:(i + 3) * chunk])) for i in range(2)])
        o_s[m] = total[:, :e]
        d_s[m] = total[:, e:]
        t_s[m] = jnp.broadcast_to(top, (rows, e))

    def rims(b, n):
        return cat(ends[1, max(b - 1, 0), n], ends[0, min(b + 1, last), n])

    def near_scores(b):
        q = qp[:, b].reshape(rows, e)
        k_rim = rims(b, 0)
        own = nt(q, kv[1, :, 0, b].reshape(rows, e)) + near_bias[:, :rows]
        rim = nt(q, k_rim) + near_bias[:, rows:]
        if b == 0:
            rim += bias(lane >= SIDE)
        if b == last:
            rim += bias(lane < SIDE)
        return own, rim

    def near(b, own, rim):
        vb, v_rim = kv[1, :, 1, b].reshape(rows, e), rims(b, 1)
        at_b = pl.ds(b * chunk, chunk)
        old = t_s[:, at_b].reshape(rows, e)
        peak = jnp.maximum(jnp.maximum(own[:, :e], own[:, e:]), rim)
        top = jnp.maximum(old, jnp.max(peak, axis=-1, keepdims=True))
        fade = jnp.exp2((old - top) * SCALE)
        both = jnp.concatenate([top, top], axis=1)
        total = nn(prob(own, both), with_ones(vb)) + nn(prob(rim, top), with_ones(v_rim))
        o_s[:, at_b] = (fade * o_s[:, at_b].reshape(rows, e) + total[:, :e]).reshape(MID, chunk, e)
        d_s[:, at_b] = (fade * d_s[:, at_b].reshape(rows, e) + total[:, e:]).reshape(MID, chunk, e)
        t_s[:, at_b] = top.reshape(MID, chunk, e)

    def far_scores(m):
        q = qp[m].reshape(rows, e)
        k2 = [[kv[i, m, n].reshape(rows, e) for n in range(2)] for i in (0, 2, 1)]
        k_far, v_far = ([cat(*x) for x in zip(*(classes(k2[i][n]) for i in range(3)))] for n in range(2))
        far = [nt(a, b) for a, b in zip(classes(q), k_far)]
        far, own = unclass([x[:, :e] + far_bias[...] for x in far]), unclass([x[:, e:] for x in far])
        k_rim, v_rim = (cat(k2[0][n][last * chunk:], k2[1][n][:chunk], outer[n]) for n in range(2))
        rim = nt(cat(q[:chunk], q[last * chunk:]), k_rim) + rim_bias[m]
        return far, own, rim, v_far, v_rim

    def other_planes(m, far, own, rim, v_far, v_rim):
        peak = jnp.maximum(rim[:, :e], rim[:, e:])
        peak = cat(jnp.maximum(far[:chunk], peak[:chunk]), far[chunk:last * chunk],
                   jnp.maximum(far[last * chunk:], peak[chunk:]))
        old = t_s[m]
        top = jnp.maximum(old, jnp.maximum(
            jnp.max(peak, axis=-1, keepdims=True), jnp.max(own, axis=-1, keepdims=True)))
        fade = jnp.exp2((old - top) * SCALE)
        p4 = jnp.concatenate([prob(far, top), prob(own, top[:, :chunk])], axis=1).reshape(MID, NS, mm, 3 * chunk)
        total = unclass([nn(p4[:, n].reshape(chunk, 3 * chunk), with_ones(v)) for n, v in enumerate(v_far)])
        top = cat(top[:chunk], top[last * chunk:])
        extra = nn(prob(rim, jnp.concatenate([top, top], axis=1)), with_ones(v_rim))
        total = cat(total[:chunk] + extra[:chunk], total[chunk:last * chunk], total[last * chunk:] + extra[chunk:])
        o = fade * o_s[m] + total[:, :e]
        den = fade * d_s[m] + total[:, e:]
        ob[m] = (o / den).astype(BF16).reshape(MID, chunk, e)

    def cols(core, head):
        return pl.ds(pl.multiple_of(core * width + head * e, e), e)

    def side(core):
        return pl.ds(pl.multiple_of(core * width, width), width)

    def result(m, d):
        return remote(ob.at[m, others[d]], att.at[m, :, cols(c, j)], res_s.at[0], res_r.at[m], mate(d), c)

    def across(m, b, to):
        return remote(ob.at[m, b], att.at[m, :, cols(c, j)], cross_s.at[0], cross_r.at[m - EARLY], to, 1 - c)

    def share(m):
        return remote(att.at[m, :, side(c)], att.at[m, :, side(c)], tp_s.at[0], tp_r.at[max(m - EARLY + 1, 0)], p, 1 - c)

    early = tuple(range(EARLY))
    late = tuple(range(EARLY, MID))

    def finish(ms):
        @pl.when(has_dn)
        def _():
            for m in ms:
                await_all(kv.at[0, m, :, pl.ds(0, last)], up_r.at[m])

        @pl.when(has_up)
        def _():
            for m in ms:
                await_all(kv.at[2, m, :, pl.ds(1, last)], dn_r.at[m])

        if ms[0] == 0:
            find_outer()
        scores = [far_scores(m) for m in ms]
        for m, x in zip(ms, scores):
            other_planes(m, *x)
        for m in ms:
            for d in range(last):
                result(m, d).start()
            if m in late:
                @pl.when(c == 0)
                def _():
                    for d in range(last):
                        across(m, others[d], mate(d)).start()
                    across(m, j, p).start()
            att[m, :, cols(c, j)] = ob[m, pl.ds(j, 1)].reshape(chunk, e)

    def half_of(ms, core):
        x = att[ms[0]:ms[-1] + 1, :, side(core)].reshape(len(ms) * chunk, width)
        return nn(x, w_in[side(core), :])

    def begin(ms, core):
        partial[ms[0] * chunk:(ms[-1] + 1) * chunk] = half_of(ms, core)

    def complete(ms, y):
        for i, m in enumerate(ms):
            for n in range(NS):
                part = y[i * chunk + n * mm:i * chunk + (n + 1) * mm]
                for t in range(natural.shape[0]):
                    natural[t, pl.ds(MID * n + m, mm, stride=FAR), :] = part[:, t * e:(t + 1) * e]

    def end(ms, core):
        complete(ms, partial[ms[0] * chunk:(ms[-1] + 1) * chunk] + half_of(ms, core))

    for d in (1, 2, 0):
        b = others[d]
        await_all(kv.at[1, 0, :, b], give_r.at[b])

        @pl.when(has_up)
        def _():
            up(0, b).start()

        @pl.when(has_dn)
        def _():
            down(0, b).start()

    def arrival(m):
        await_all(kv.at[1, m, :, pl.ds(0, last)], give_r.at[last + m])

    arrival(1)
    for b in range(MID):
        relay(1, b, True, True)
    for m in range(2, MID):
        arrival(m)
        relay(m, last, True, False)
        relay(m, 0, False, True)
    def relay_rest(m):
        for b in range(MID):
            relay(m, b, b != last, b != 0)

    relay_rest(2)
    pl.when(c == 0)(functools.partial(relay_rest, 3))
    find_ends()
    await_all(qp.at[pl.ds(0, 2), pl.ds(0, last)], ask_r.at[0])
    pl.when(c == 1)(functools.partial(relay_rest, 3))
    middle(0)
    middle(1)
    await_all(qp.at[pl.ds(0, 2), pl.ds(0, last)], ask_r.at[1])
    middle(2)
    scores = near_scores(0)
    middle(3)
    for b in range(MID):
        now, scores = scores, near_scores(b + 1) if b < last else None
        near(b, *now)
    @pl.when(has_dn)
    def _():
        await_all(kv.at[0, :, :, last], up_r.at[MID])

    @pl.when(has_up)
    def _():
        await_all(kv.at[2, :, :, 0], dn_r.at[MID])

    finish((0, 1))
    finish((2,))
    finish((3,))
    for m in early:
        await_all(ob.at[m, pl.ds(0, last)], res_r.at[m])
        share(m).start()
    loads[3].wait()
    @pl.when(c == 0)
    def _():
        begin(early, 0)
        await_all(att.at[pl.ds(0, EARLY), :, side(1)], tp_r.at[0])
        end(early, 1)
        for m in late:
            await_all(att.at[m, :, side(1)], tp_r.at[m - EARLY + 1])
        begin(late, 1)
        for m in late:
            await_all(ob.at[m, pl.ds(0, last)], res_r.at[m])
            end((m,), 0)

    @pl.when(c == 1)
    def _():
        for m in late:
            await_all(ob.at[m, pl.ds(0, last)], res_r.at[m])
            share(m).start()
        begin(tuple(range(MID)), 1)
        await_all(ob.at[late[0]], cross_r.at[0])
        end(late[:1], 0)
        await_all(att.at[pl.ds(0, EARLY), :, side(0)], tp_r.at[0])
        end(early, 0)
        for m in late[1:]:
            await_all(ob.at[m], cross_r.at[m - EARLY])
            end((m,), 0)

    for t in range(natural.shape[0]):
        out_ref[:, t * e:(t + 1) * e] = natural[t].astype(BF16)

    await_all(ps.at[:, pl.ds(0, last), pair], give_s.at[0])
    await_all(ps.at[:, pl.ds(0, last), 2], ask_s.at[0])
    await_all(ob.at[:, pl.ds(0, last)], res_s.at[0])

    @pl.when(c == 0)
    def _():
        await_all(ob.at[pl.ds(0, MID - EARLY)], cross_s.at[0])
        await_all(att.at[pl.ds(0, EARLY), :, side(c)], tp_s.at[0])

    @pl.when(c == 1)
    def _():
        await_all(att.at[:, :, side(c)], tp_s.at[0])

    @pl.when(has_up)
    def _():
        await_all(kv.at[0], up_s.at[0])

    @pl.when(has_dn)
    def _():
        await_all(kv.at[2], dn_s.at[0])


def per_device(sp_n, q, k, v, w):
    rows, columns = q.shape
    heads = columns // HEAD_DIM
    assert MID * rows == SIDE * FAR and rows // MID == SIDE and sp_n % MID == 0 and heads == MID
    dma = pltpu.SemaphoreType.DMA
    e, chunk = HEAD_DIM, rows // MID
    vmem = lambda *shape, dtype=BF16: pltpu.VMEM(shape, dtype)
    pinned = [pltpu.with_memory_space_constraint(x, pltpu.HBM) for x in (q, k, v, w)]
    return pl.pallas_call(
        functools.partial(kernel, sp_n, heads),
        out_shape=pltpu.VMEM((rows, w.shape[1]), BF16),
        in_specs=[pl.BlockSpec(memory_space=pltpu.HBM)] * 4,
        out_specs=pl.BlockSpec(memory_space=pltpu.VMEM),
        scratch_shapes=[
            vmem(rows, columns), vmem(rows, columns), vmem(rows, columns), vmem(*w.shape),
            vmem(MID, heads, 3, chunk, e),
            vmem(3, MID, 2, MID, chunk, e),
            vmem(MID, MID, chunk, e),
            vmem(2, MID, 2, SIDE, e),
            vmem(2, 2 * SIDE, e),
            vmem(rows, rows + 2 * SIDE, dtype=F32),
            vmem(2, rows // 2, 3 * chunk, dtype=F32),
            vmem(chunk, 2 * chunk, dtype=F32),
            vmem(MID, rows // 2, 4 * chunk, dtype=F32),
            vmem(MID, rows, e, dtype=F32), vmem(MID, rows, e, dtype=F32), vmem(MID, rows, e, dtype=F32),
            vmem(MID, MID, chunk, e),
            vmem(MID, chunk, 2 * columns),
            vmem(rows, w.shape[1], dtype=F32),
            vmem(w.shape[1] // e, rows, e, dtype=F32),
            dma((4,)),
            dma((1,)), dma((2 * MID - 1,)),
            dma((1,)), dma((2,)),
            dma((1,)), dma((MID + 1,)),
            dma((1,)), dma((MID + 1,)),
            dma((1,)), dma((MID,)),
            dma((1,)), dma((MID - EARLY,)),
            dma((1,)), dma((MID - EARLY + 1,)),
        ],
        compiler_params=pltpu.CompilerParams(
            collective_id=0, has_side_effects=True, vmem_limit_bytes=40 * 1024 * 1024),
    )(*pinned)


def solution(mesh):
    return jax.shard_map(
        functools.partial(per_device, mesh.shape["sp"]), mesh=mesh,
        in_specs=(P("sp", "tp"), P("sp", "tp"), P("sp", "tp"), P(None, "tp")),
        out_specs=P("sp", "tp"), check_vma=False,
    )
```

```python
import functools
import math

import jax
import jax.numpy as jnp
from jax import lax
from jax.experimental import pallas as pl
from jax.experimental.pallas import tpu as pltpu
from jax.sharding import PartitionSpec as P

HEAD_DIM = 128
SIDE = 64
MID = 4
FAR = 16
NS = FAR // MID
MESH = pl.DeviceIdType.MESH
F32 = jnp.float32
BF16 = jnp.bfloat16
SCALE = HEAD_DIM ** -0.5 * math.log2(math.e)
NEG = -jnp.inf
EARLY = 2


def nt(a, b):
    return lax.dot_general(a, b, (((1,), (1,)), ((), ())), preferred_element_type=F32)


def nn(a, b):
    return lax.dot_general(a, b, (((1,), (0,)), ((), ())), preferred_element_type=F32)


def iota(shape, dim):
    return lax.broadcasted_iota(jnp.int32, shape, dim)


def bias(ok):
    return jnp.where(ok, 0.0, NEG).astype(F32)


def kernel(sp_n, heads, q_hbm, k_hbm, v_hbm, w_hbm, out_ref,
           q_in, k_in, v_in, w_in, ps, kv, qp, ends, outer, near_bias, mid_bias, far_bias, rim_bias,
           o_s, t_s, d_s, ob, att, partial, natural,
           load_sem, give_s, give_r, ask_s, ask_r, up_s, up_r, dn_s, dn_r, res_s, res_r, cross_s, cross_r, tp_s, tp_r):
    rows = q_in.shape[0]
    chunk = rows // MID
    mm = rows // FAR
    e = HEAD_DIM
    width = heads * e
    last = MID - 1
    p, c = lax.axis_index("sp"), lax.axis_index("tp")
    groups = sp_n // MID
    g, j = p // MID, p % MID

    loads = [
        pltpu.make_async_copy(src, dst, load_sem.at[n])
        for n, (src, dst) in enumerate(((k_hbm, k_in), (v_hbm, v_in), (q_hbm, q_in), (w_hbm, w_in)))
    ]
    for load in loads[:3]:
        load.start()

    barrier = pltpu.get_barrier_semaphore()

    def greet(sp, tp):
        pl.semaphore_signal(barrier, inc=1, device_id=(sp, tp), device_id_type=MESH)

    others = (MID - 1 - j, j + 1 - 2 * (j % 2), (j + MID // 2) % MID)

    def mate(d):
        return g * MID + others[d]

    for d in range(last):
        greet(mate(d), c)
        greet(mate(d), 1 - c)
    greet(p, 1 - c)
    has_dn, has_up = g > 0, g < groups - 1
    up_p, dn_p = (p + MID) % sp_n, (p - MID + sp_n) % sp_n

    @pl.when(has_dn)
    def _():
        greet(dn_p, c)

    @pl.when(has_up)
    def _():
        greet(up_p, c)

    def remote(src, dst, ss, rs, sp, tp):
        return pltpu.make_async_remote_copy(
            src_ref=src, dst_ref=dst, send_sem=ss, recv_sem=rs, device_id=(sp, tp), device_id_type=MESH)

    def await_all(ref, sem):
        pltpu.make_async_copy(ref, ref, sem).wait()

    def token(r):
        return FAR * (r % mm) + MID * ((r % chunk) // mm) + r // chunk

    r, t = iota((rows, rows), 0), iota((rows, rows), 1)
    perm = (t == token(r)).astype(BF16)

    def reorder(*arrays):
        for n, _ in arrays:
            loads[n].wait()
        for n, x in arrays:
            moved = nn(perm, x[...]).astype(BF16)
            for h in range(heads):
                for m in range(MID):
                    ps[m, h, n] = moved[m * chunk:(m + 1) * chunk, h * e:(h + 1) * e]

    reorder((0, k_in), (1, v_in))

    @pl.when(jnp.logical_not(has_dn))
    def _():
        kv[0] = jnp.zeros(kv.shape[1:], BF16)

    @pl.when(jnp.logical_not(has_up))
    def _():
        kv[2] = jnp.zeros(kv.shape[1:], BF16)

    pl.semaphore_wait(barrier, 2 * MID - 1 + has_dn.astype(jnp.int32) + has_up.astype(jnp.int32))

    pair = pl.ds(0, 2)

    def give(m, d):
        return remote(ps.at[m, others[d], pair], kv.at[1, m, :, j], give_s.at[0], give_r.at[j if m == 0 else last + m], mate(d), c)

    def ask(i, d):
        two = pl.ds(2 * i, 2)
        return remote(ps.at[two, others[d], 2], qp.at[two, j], ask_s.at[0], ask_r.at[i], mate(d), c)

    def up(m, b, own=False):
        src = ps.at[m, j, pair] if own else kv.at[1, m, :, b]
        edge = (b == last).astype(jnp.int32) if hasattr(b, "astype") else int(b == last)
        arrived = edge * MID + (1 - edge) * m
        return remote(src, kv.at[0, m, :, b], up_s.at[0], up_r.at[arrived], up_p, c)

    def down(m, b, own=False):
        src = ps.at[m, j, pair] if own else kv.at[1, m, :, b]
        edge = (b == 0).astype(jnp.int32) if hasattr(b, "astype") else int(b == 0)
        arrived = edge * MID + (1 - edge) * m
        return remote(src, kv.at[2, m, :, b], dn_s.at[0], dn_r.at[arrived], dn_p, c)

    for m in range(MID):
        for d in ((1, 2, 0) if m == 0 else range(last)):
            give(m, d).start()
        if m == 0:
            @pl.when(has_up)
            def _():
                for i in range(MID):
                    up(i, j, own=True).start()

            @pl.when(has_dn)
            def _():
                for i in range(MID):
                    down(i, j, own=True).start()

    reorder((2, q_in))
    for i in range(2):
        for d in range(last):
            ask(i, d).start()

    loads[3].start()
    for m in range(MID):
        kv[1, m, :, pl.ds(j, 1)] = ps[m, pl.ds(j, 1), 0:2].reshape(2, 1, chunk, e)
        qp[m, pl.ds(j, 1)] = ps[m, pl.ds(j, 1), 2]

    ok_dn, ok_up = has_dn.astype(jnp.int32) == 1, has_up.astype(jnp.int32) == 1
    tq, s = token(iota((rows, rows), 0)), iota((rows, rows), 1)
    gap = tq - token(s)
    near_bias[:, :rows] = bias((gap >= -SIDE) & (gap <= SIDE))
    tq, s = token(iota((rows, 2 * SIDE), 0)), iota((rows, 2 * SIDE), 1)
    near_bias[:, rows:] = bias(((s < SIDE) & (s >= tq)) | ((s >= SIDE) & (s - SIDE <= tq - (rows - SIDE))))

    def order(x):
        return chunk * (x // chunk) + NS * (x % mm) + (x % chunk) // mm

    half = rows // 2
    uq, uk = order(iota((half, 3 * chunk), 0)), order(iota((half, 3 * chunk), 1))
    for i in range(2):
        gap = uk - uq - i * chunk
        mid_bias[i] = bias((gap >= -SIDE) & (gap <= SIDE))
    x, s = iota((chunk, 2 * chunk), 0), iota((chunk, 2 * chunk), 1)
    far_bias[...] = bias(((s < chunk) & (s >= x) & ok_dn) | ((s >= chunk) & (s - chunk <= x) & ok_up))
    x, s = iota((half, 2 * chunk), 0), iota((half, 2 * chunk), 1)
    u, v = order(x % chunk), order(s % chunk)
    low, high = (x < chunk) & (s < chunk) & ok_dn, (x >= chunk) & (s >= chunk) & ok_up
    for m in range(MID):
        tq = token(m * chunk + x % chunk)
        rim_bias[m, :, :2 * chunk] = bias((low & (v >= u)) | (high & (v <= u)))
        rim_bias[m, :, 2 * chunk:] = bias((low & (s >= tq)) | (high & (s - SIDE <= tq - (rows - SIDE))))

    def relay(m, b, rise, fall):
        if rise:
            @pl.when((j != b) & has_up)
            def _():
                up(m, b).start()

        if fall:
            @pl.when((j != b) & has_dn)
            def _():
                down(m, b).start()

    def classes(x):
        x4 = x.reshape(MID, NS, mm, e)
        return [x4[:, n].reshape(chunk, e) for n in range(NS)]

    def unclass(parts):
        return jnp.concatenate([parts[n][i * mm:(i + 1) * mm] for i in range(MID) for n in range(NS)], axis=0)

    def cat(*parts):
        return jnp.concatenate(parts, axis=0)

    def with_ones(x):
        return jnp.concatenate([x, jnp.ones((x.shape[0], e), BF16)], axis=1)

    def prob(s, top):
        return jnp.exp2((s - top) * SCALE).astype(BF16)

    x, s = iota((2 * SIDE, rows), 0), iota((2 * SIDE, rows), 1)
    pick = (token(s) == x + (x // SIDE) * (rows - 2 * SIDE)).astype(BF16)

    def both(i, b):
        return jnp.concatenate([kv[i, :, n, b].reshape(rows, e) for n in range(2)], axis=1)

    def find_ends():
        for b in range(MID):
            x = nn(pick, both(1, b)).astype(BF16)
            for side in range(2):
                for n in range(2):
                    ends[side, b, n] = x[side * SIDE:(side + 1) * SIDE, n * e:(n + 1) * e]

    def find_outer():
        x = cat(nn(pick[SIDE:], both(0, last)), nn(pick[:SIDE], both(2, 0))).astype(BF16)
        for n in range(2):
            outer[n] = x[:, n * e:(n + 1) * e]

    lane = iota((1, 2 * SIDE), 1)

    def middle_scores(m):
        q = qp[m].reshape(rows, e)
        kh, vh = kv[1, m, 0].reshape(rows, e), kv[1, m, 1].reshape(rows, e)
        mid = cat(*[nt(q[i * half:(i + 1) * half], kh[i * chunk:(i + 3) * chunk]) + mid_bias[i] for i in range(2)])
        return mid, vh

    def middle(m, mid, vh):
        top = jnp.maximum(jnp.max(mid[:, :e], axis=-1, keepdims=True), jnp.max(mid[:, e:], axis=-1, keepdims=True))
        p_mid = prob(mid, top)
        total = cat(*[nn(p_mid[i * half:(i + 1) * half], with_ones(vh[i * chunk:(i + 3) * chunk])) for i in range(2)])
        o_s[m] = total[:, :e]
        d_s[m] = total[:, e:]
        t_s[m] = jnp.broadcast_to(top, (rows, e))

    def rims(b, n):
        return cat(ends[1, max(b - 1, 0), n], ends[0, min(b + 1, last), n])

    def near_scores(b):
        q = qp[:, b].reshape(rows, e)
        k_rim = rims(b, 0)
        own = nt(q, kv[1, :, 0, b].reshape(rows, e)) + near_bias[:, :rows]
        rim = nt(q, k_rim) + near_bias[:, rows:]
        if b == 0:
            rim += bias(lane >= SIDE)
        if b == last:
            rim += bias(lane < SIDE)
        return own, rim

    def near(b, own, rim):
        vb, v_rim = kv[1, :, 1, b].reshape(rows, e), rims(b, 1)
        at_b = pl.ds(b * chunk, chunk)
        old = t_s[:, at_b].reshape(rows, e)
        peak = jnp.maximum(jnp.maximum(own[:, :e], own[:, e:]), rim)
        top = jnp.maximum(old, jnp.max(peak, axis=-1, keepdims=True))
        fade = jnp.exp2((old - top) * SCALE)
        both = jnp.concatenate([top, top], axis=1)
        total = nn(prob(own, both), with_ones(vb)) + nn(prob(rim, top), with_ones(v_rim))
        o_s[:, at_b] = (fade * o_s[:, at_b].reshape(rows, e) + total[:, :e]).reshape(MID, chunk, e)
        d_s[:, at_b] = (fade * d_s[:, at_b].reshape(rows, e) + total[:, e:]).reshape(MID, chunk, e)
        t_s[:, at_b] = top.reshape(MID, chunk, e)

    def far_scores(m):
        q = qp[m].reshape(rows, e)
        k2 = [[kv[i, m, n].reshape(rows, e) for n in range(2)] for i in (0, 2, 1)]
        k_far, v_far = ([cat(*x) for x in zip(*(classes(k2[i][n]) for i in range(3)))] for n in range(2))
        far = [nt(a, b) for a, b in zip(classes(q), k_far)]
        far, own = unclass([x[:, :e] + far_bias[...] for x in far]), unclass([x[:, e:] for x in far])
        k_rim, v_rim = (cat(k2[0][n][last * chunk:], k2[1][n][:chunk], outer[n]) for n in range(2))
        rim = nt(cat(q[:chunk], q[last * chunk:]), k_rim) + rim_bias[m]
        return far, own, rim, v_far, v_rim

    def other_planes(m, far, own, rim, v_far, v_rim):
        peak = jnp.maximum(rim[:, :e], rim[:, e:])
        peak = cat(jnp.maximum(far[:chunk], peak[:chunk]), far[chunk:last * chunk],
                   jnp.maximum(far[last * chunk:], peak[chunk:]))
        old = t_s[m]
        top = jnp.maximum(old, jnp.maximum(
            jnp.max(peak, axis=-1, keepdims=True), jnp.max(own, axis=-1, keepdims=True)))
        fade = jnp.exp2((old - top) * SCALE)
        p4 = jnp.concatenate([prob(far, top), prob(own, top[:, :chunk])], axis=1).reshape(MID, NS, mm, 3 * chunk)
        total = unclass([nn(p4[:, n].reshape(chunk, 3 * chunk), with_ones(v)) for n, v in enumerate(v_far)])
        top = cat(top[:chunk], top[last * chunk:])
        extra = nn(prob(rim, jnp.concatenate([top, top], axis=1)), with_ones(v_rim))
        total = cat(total[:chunk] + extra[:chunk], total[chunk:last * chunk], total[last * chunk:] + extra[chunk:])
        o = fade * o_s[m] + total[:, :e]
        den = fade * d_s[m] + total[:, e:]
        ob[m] = (o / den).astype(BF16).reshape(MID, chunk, e)

    def cols(core, head):
        return pl.ds(pl.multiple_of(core * width + head * e, e), e)

    def side(core):
        return pl.ds(pl.multiple_of(core * width, width), width)

    def result(m, d):
        return remote(ob.at[m, others[d]], att.at[m, :, cols(c, j)], res_s.at[0], res_r.at[m], mate(d), c)

    def across(m, b, to):
        return remote(ob.at[m, b], att.at[m, :, cols(c, j)], cross_s.at[0], cross_r.at[m - EARLY], to, 1 - c)

    def share(m):
        return remote(att.at[m, :, side(c)], att.at[m, :, side(c)], tp_s.at[0], tp_r.at[max(m - EARLY + 1, 0)], p, 1 - c)

    early = tuple(range(EARLY))
    late = tuple(range(EARLY, MID))

    def finish(ms):
        @pl.when(has_dn)
        def _():
            for m in ms:
                await_all(kv.at[0, m, :, pl.ds(0, last)], up_r.at[m])

        @pl.when(has_up)
        def _():
            for m in ms:
                await_all(kv.at[2, m, :, pl.ds(1, last)], dn_r.at[m])

        if ms[0] == 0:
            find_outer()
        scores = [far_scores(m) for m in ms]
        for m, x in zip(ms, scores):
            other_planes(m, *x)
        for m in ms:
            for d in range(last):
                result(m, d).start()
            if m in late:
                @pl.when(c == 0)
                def _():
                    for d in range(last):
                        across(m, others[d], mate(d)).start()
                    across(m, j, p).start()
            att[m, :, cols(c, j)] = ob[m, pl.ds(j, 1)].reshape(chunk, e)

    def half_of(ms, core):
        x = att[ms[0]:ms[-1] + 1, :, side(core)].reshape(len(ms) * chunk, width)
        return nn(x, w_in[side(core), :])

    def begin(ms, core):
        partial[ms[0] * chunk:(ms[-1] + 1) * chunk] = half_of(ms, core)

    def complete(ms, y):
        for i, m in enumerate(ms):
            for n in range(NS):
                part = y[i * chunk + n * mm:i * chunk + (n + 1) * mm]
                for t in range(natural.shape[0]):
                    natural[t, pl.ds(MID * n + m, mm, stride=FAR), :] = part[:, t * e:(t + 1) * e]

    def end(ms, core):
        complete(ms, partial[ms[0] * chunk:(ms[-1] + 1) * chunk] + half_of(ms, core))

    for d in (1, 2, 0):
        b = others[d]
        await_all(kv.at[1, 0, :, b], give_r.at[b])

        @pl.when(has_up)
        def _():
            up(0, b).start()

        @pl.when(has_dn)
        def _():
            down(0, b).start()

    def arrival(m):
        await_all(kv.at[1, m, :, pl.ds(0, last)], give_r.at[last + m])

    arrival(1)
    for b in range(MID):
        relay(1, b, True, True)
    for m in range(2, MID):
        arrival(m)
        relay(m, last, True, False)
        relay(m, 0, False, True)
    def relay_rest(m):
        for b in range(MID):
            relay(m, b, b != last, b != 0)

    relay_rest(2)
    pl.when(c == 0)(functools.partial(relay_rest, 3))
    find_ends()
    await_all(qp.at[pl.ds(0, 2), pl.ds(0, last)], ask_r.at[0])
    pl.when(c == 1)(functools.partial(relay_rest, 3))
    for m, x in enumerate([middle_scores(0), middle_scores(1)]):
        middle(m, *x)
    await_all(qp.at[pl.ds(0, 2), pl.ds(0, last)], ask_r.at[1])
    two = [middle_scores(2), middle_scores(3)]
    middle(2, *two[0])
    scores = near_scores(0)
    middle(3, *two[1])
    for b in range(MID):
        now, scores = scores, near_scores(b + 1) if b < last else None
        near(b, *now)
    @pl.when(has_dn)
    def _():
        await_all(kv.at[0, :, :, last], up_r.at[MID])

    @pl.when(has_up)
    def _():
        await_all(kv.at[2, :, :, 0], dn_r.at[MID])

    finish((0, 1))
    finish((2,))
    finish((3,))
    for m in early:
        await_all(ob.at[m, pl.ds(0, last)], res_r.at[m])
        share(m).start()
    loads[3].wait()
    @pl.when(c == 0)
    def _():
        begin(early, 0)
        await_all(att.at[pl.ds(0, EARLY), :, side(1)], tp_r.at[0])
        end(early, 1)
        for m in late:
            await_all(att.at[m, :, side(1)], tp_r.at[m - EARLY + 1])
        begin(late, 1)
        for m in late:
            await_all(ob.at[m, pl.ds(0, last)], res_r.at[m])
            end((m,), 0)

    @pl.when(c == 1)
    def _():
        for m in late:
            await_all(ob.at[m, pl.ds(0, last)], res_r.at[m])
            share(m).start()
        begin(tuple(range(MID)), 1)
        await_all(ob.at[late[0]], cross_r.at[0])
        end(late[:1], 0)
        await_all(att.at[pl.ds(0, EARLY), :, side(0)], tp_r.at[0])
        end(early, 0)
        for m in late[1:]:
            await_all(ob.at[m], cross_r.at[m - EARLY])
            end((m,), 0)

    for t in range(natural.shape[0]):
        out_ref[:, t * e:(t + 1) * e] = natural[t].astype(BF16)

    await_all(ps.at[:, pl.ds(0, last), pair], give_s.at[0])
    await_all(ps.at[:, pl.ds(0, last), 2], ask_s.at[0])
    await_all(ob.at[:, pl.ds(0, last)], res_s.at[0])

    @pl.when(c == 0)
    def _():
        await_all(ob.at[pl.ds(0, MID - EARLY)], cross_s.at[0])
        await_all(att.at[pl.ds(0, EARLY), :, side(c)], tp_s.at[0])

    @pl.when(c == 1)
    def _():
        await_all(att.at[:, :, side(c)], tp_s.at[0])

    @pl.when(has_up)
    def _():
        await_all(kv.at[0], up_s.at[0])

    @pl.when(has_dn)
    def _():
        await_all(kv.at[2], dn_s.at[0])


def per_device(sp_n, q, k, v, w):
    rows, columns = q.shape
    heads = columns // HEAD_DIM
    assert MID * rows == SIDE * FAR and rows // MID == SIDE and sp_n % MID == 0 and heads == MID
    dma = pltpu.SemaphoreType.DMA
    e, chunk = HEAD_DIM, rows // MID
    vmem = lambda *shape, dtype=BF16: pltpu.VMEM(shape, dtype)
    pinned = [pltpu.with_memory_space_constraint(x, pltpu.HBM) for x in (q, k, v, w)]
    return pl.pallas_call(
        functools.partial(kernel, sp_n, heads),
        out_shape=pltpu.VMEM((rows, w.shape[1]), BF16),
        in_specs=[pl.BlockSpec(memory_space=pltpu.HBM)] * 4,
        out_specs=pl.BlockSpec(memory_space=pltpu.VMEM),
        scratch_shapes=[
            vmem(rows, columns), vmem(rows, columns), vmem(rows, columns), vmem(*w.shape),
            vmem(MID, heads, 3, chunk, e),
            vmem(3, MID, 2, MID, chunk, e),
            vmem(MID, MID, chunk, e),
            vmem(2, MID, 2, SIDE, e),
            vmem(2, 2 * SIDE, e),
            vmem(rows, rows + 2 * SIDE, dtype=F32),
            vmem(2, rows // 2, 3 * chunk, dtype=F32),
            vmem(chunk, 2 * chunk, dtype=F32),
            vmem(MID, rows // 2, 4 * chunk, dtype=F32),
            vmem(MID, rows, e, dtype=F32), vmem(MID, rows, e, dtype=F32), vmem(MID, rows, e, dtype=F32),
            vmem(MID, MID, chunk, e),
            vmem(MID, chunk, 2 * columns),
            vmem(rows, w.shape[1], dtype=F32),
            vmem(w.shape[1] // e, rows, e, dtype=F32),
            dma((4,)),
            dma((1,)), dma((2 * MID - 1,)),
            dma((1,)), dma((2,)),
            dma((1,)), dma((MID + 1,)),
            dma((1,)), dma((MID + 1,)),
            dma((1,)), dma((MID,)),
            dma((1,)), dma((MID - EARLY,)),
            dma((1,)), dma((MID - EARLY + 1,)),
        ],
        compiler_params=pltpu.CompilerParams(
            collective_id=0, has_side_effects=True, vmem_limit_bytes=40 * 1024 * 1024),
    )(*pinned)


def solution(mesh):
    return jax.shard_map(
        functools.partial(per_device, mesh.shape["sp"]), mesh=mesh,
        in_specs=(P("sp", "tp"), P("sp", "tp"), P("sp", "tp"), P(None, "tp")),
        out_specs=P("sp", "tp"), check_vma=False,
    )
```
